32 devices in a mesh: grp: 2 (over x), ep: 16 (over z, y, core).
Axes of the slice: x: 2, y: 2, z: 4, core: 2. Of those that a mesh axis runs over, the one named last changes fastest.
Arguments:
- resid: bfloat16 [384, 2048], P(('grp', 'ep')), parts along dimension 0, may hold values from -6 to 6
- norm_gains: float32 [4, 2048], replicated, may hold values from 0.1 to 1.9
- w_query: bfloat16 [2048, 1024], P(None, 'ep'), may hold values from -0.125 to 0.125
- w_key: bfloat16 [2048, 1024], P(None, 'ep'), may hold values from -0.125 to 0.125
- w_value: bfloat16 [2048, 1024], P(None, 'ep'), may hold values from -0.125 to 0.125
- w_outgate: bfloat16 [2048, 1024], P(None, 'ep'), may hold values from -0.125 to 0.125
- w_igate: bfloat16 [2048, 8], replicated, may hold values from -0.125 to 0.125
- w_fgate: bfloat16 [2048, 8], replicated, may hold values from -0.125 to 0.125
- igate_bias: float32 [8], replicated, may hold values from -1 to 1
- fgate_bias: float32 [8], replicated, may hold values from -1 to 5
- state_matrix: float32 [384, 8, 128, 128], P(('grp', 'ep')), parts along dimension 0, may hold values from -0.8 to 0.8
- state_norm: float32 [384, 8, 128], P(('grp', 'ep')), parts along dimension 0, may hold values from -2.4 to 2.4
- state_max: float32 [384, 8], P(('grp', 'ep')), parts along dimension 0, may hold values from -1 to 1
- w_mix_out: bfloat16 [1024, 2048], replicated, may hold values from -0.1875 to 0.1875
- routes: int32 [384, 2], P(('grp', 'ep')), parts along dimension 0, may hold values from 0 to 15, all different within a row; in each aligned block of 12 rows (0 to 11, 12 to 23, ...) at most 2 rows name the same one
- route_scores: bfloat16 [384, 2], P(('grp', 'ep')), parts along dimension 0, may hold values from 0.099609375 to 1
- expert_gate: bfloat16 [16, 2048, 512], P('ep'), may hold values from -0.125 to 0.125
- expert_up: bfloat16 [16, 2048, 512], P('ep'), may hold values from -0.125 to 0.125
- expert_down: bfloat16 [16, 512, 2048], P('ep'), may hold values from -0.25 to 0.25
- dense_gate: bfloat16 [2048, 8192], P(None, 'ep'), may hold values from -0.125 to 0.125
- dense_up: bfloat16 [2048, 8192], P(None, 'ep'), may hold values from -0.125 to 0.125
- dense_down: bfloat16 [8192, 2048], P('ep'), may hold values from -0.0625 to 0.0625
- branch_weight: bfloat16 [2048], replicated, may hold values from -0.125 to 0.125
Outputs:
- out_stream: bfloat16 [384, 2048], P(('grp', 'ep')), parts along dimension 0
- new_matrix: float32 [384, 8, 128, 128], P(('grp', 'ep')), parts along dimension 0
- new_norm: float32 [384, 8, 128], P(('grp', 'ep')), parts along dimension 0
- new_max: float32 [384, 8], P(('grp', 'ep')), parts along dimension 0
The draws below stay inside these ranges and needn't reach their ends.
There are 2 independent parts, one for each index of `grp`. The reference program is written for one: setup_inputs(seed, part) draws one part's arguments, and reference() takes and returns one part's arrays. A program takes and returns all parts, laid end to end along the dimension named above; an argument that names none is the same for every part. Nothing has to cross between parts.
Inputs may be any that keep to these rules, and one draw needn't show every extreme that they name: `routes`: each row names 2 different experts. In each aligned block of 12 rows (the rows of one device) no expert is named by more than 2 rows, a bound that some block reaches.
All inputs are finite; a program needn't handle non-finite values.
Results may differ from the reference program's by a relative error of at most 0.015.
Values may be sent and summed in bfloat16 or wider, within the bound.
A program may use at most 128 MiB of HBM per device.

```python
import math
import jax
import jax.numpy as jnp
import numpy as np
from jax import lax

D = 2048
NH = 8
DH = 128
FE = 512
FFD = 8192
TOPK = 2
SEQ_DEV = 12
INNER = 1024
CAP = 2
EXPERTS = 16
SEQS = 192
N_EP = 16


def steps_of(stream_key, shape, cuts, low, largest):
    factor_of, own = 1.0, jax.random.fold_in(stream_key, 6)
    for position, blocks in cuts:
        heights = jnp.exp(jax.random.uniform(jax.random.fold_in(own, position), (blocks,), jnp.float32, low / len(cuts), largest / len(cuts)))
        factor_of = factor_of * jnp.repeat(heights, shape[position] // blocks).reshape([-1 if axis == position else 1 for axis in range(len(shape))])
    return factor_of


def shared_out(own_key, own, number, rows, number_of, top, most, skew):
    ranking = jax.random.permutation(own_key, number_of)
    heavy_load, ordinary = portions_of(number_of, rows * top, most, skew, True), portions_of(number_of, rows * top, most, skew, False)
    places = jnp.arange(number_of)

    def named(sizes, turn):
        used = int((sizes > 0).sum())
        fixed = max(1, used // 4)
        moved = fixed + (places - fixed + turn * (used - fixed)) % max(1, number_of - fixed)
        return jnp.zeros((number_of,), jnp.int32).at[ranking[jnp.where(places < fixed, places, moved)]].set(jnp.asarray(sizes, jnp.int32))

    sizes = jnp.where(number % 4 == 0, named(heavy_load, number // 4), named(ordinary, number - number // 4 - 1))
    mixed = jax.random.permutation(jax.random.fold_in(own, 3), number_of)
    source_of, taker = mixed[0:number_of // 2 * 2:2], mixed[1:number_of // 2 * 2:2]
    slack = jnp.minimum(sizes[source_of] - 1, most - sizes[taker]) // 2
    slack = jnp.where((source_of == ranking[0]) | (taker == ranking[0]) | (sizes[taker] == 0), 0, jnp.maximum(slack, 0))
    moved = jax.random.randint(jax.random.fold_in(own, 4), (number_of // 2,), 0, 1 << 20) % (slack + 1)
    sizes = sizes.at[source_of].add(-moved).at[taker].add(moved)
    items = jnp.searchsorted(jnp.cumsum(sizes), jnp.arange(rows * top), side="right").astype(jnp.int32)
    table = items.reshape(top, rows).T
    table = table[jax.random.permutation(jax.random.fold_in(own, 1), rows)]
    turn = jax.random.randint(jax.random.fold_in(own, 2), (rows, 1), 0, top)
    return jnp.take_along_axis(table, (jnp.arange(top)[None, :] + turn) % top, axis=1)


def portions_of(number_of, total, limit, skew, full):
    loads = [(1 << 20) // math.isqrt(standing ** skew) + 1 for standing in range(1, number_of + 1)]
    largest = limit if full else min(limit, max(-(-total // number_of), total * loads[0] // sum(loads)))
    least = 1 if total - largest >= number_of - 1 else 0
    counts, spare = [largest] + [least] * (number_of - 1), total - largest - least * (number_of - 1)
    while spare > 0:
        candidates = [i for i in range(1, number_of) if counts[i] < largest] or [i for i in range(1, number_of) if counts[i] < limit]
        pool, left = sum([loads[i] for i in candidates]), spare
        for i in candidates:
            more = min(limit - counts[i], max(1, left * loads[i] // pool), spare)
            counts[i] = counts[i] + more
            spare = spare - more
    return np.array(counts)


def gaussian(rng, extent, scale, limit, cuts=(), kind=jnp.bfloat16):
    values = scale * jax.random.normal(rng, extent, jnp.float32)
    if cuts:
        values = values * steps_of(rng, extent, cuts, -0.22, 0.18)
    return jnp.clip(values, -limit, limit).astype(kind)


def setup_inputs(seed: int = 0, part: int = 0) -> dict:
    splits = jax.random.split(jax.random.key(seed), 24)
    own_keys = jax.random.split(jax.random.fold_in(splits[23], part), 24)
    resid = gaussian(own_keys[0], (SEQS, D), 1.0, 6.0, ((0, 16),))
    norm_gains = jnp.clip(1.0 + 0.18 * jax.random.normal(splits[1], (4, D), jnp.float32), 0.1, 1.9)
    w_query = gaussian(splits[2], (D, INNER), D ** -0.5, 0.125, ((1, 16),))
    w_key = gaussian(splits[3], (D, INNER), D ** -0.5, 0.125, ((1, 16),))
    w_value = gaussian(splits[4], (D, INNER), D ** -0.5, 0.125, ((1, 16),))
    w_outgate = gaussian(splits[5], (D, INNER), D ** -0.5, 0.125, ((1, 16),))
    w_igate = gaussian(splits[6], (D, NH), D ** -0.5, 0.125)
    w_fgate = gaussian(splits[7], (D, NH), D ** -0.5, 0.125)
    igate_bias = jnp.clip(jax.random.uniform(splits[8], (NH,), jnp.float32, -1.0, 1.0), -1.0, 1.0)
    fgate_bias = jnp.clip(jax.random.uniform(splits[9], (NH,), jnp.float32, -1.0, 5.0), -1.0, 5.0)
    state_matrix = gaussian(own_keys[10], (SEQS, NH, DH, DH), 0.1, 0.8, ((0, 16),), jnp.float32)
    state_norm = gaussian(own_keys[11], (SEQS, NH, DH), 0.3, 2.4, ((0, 16),), jnp.float32)
    state_max = jnp.clip(jax.random.uniform(own_keys[12], (SEQS, NH), jnp.float32, -1.0, 1.0) * steps_of(own_keys[12], (SEQS, NH), ((0, 16),), -0.4, 0.0), -1.0, 1.0)
    w_mix_out = gaussian(splits[13], (INNER, D), INNER ** -0.5, 0.1875)
    routes_keys = jax.random.split(jax.random.fold_in(own_keys[14], 1), SEQS // SEQ_DEV)
    routes_turns = jax.random.permutation(jax.random.fold_in(own_keys[14], 3), SEQS // SEQ_DEV)
    routes = jax.vmap(lambda own, number: shared_out(jax.random.fold_in(own_keys[14], 2), own, number, SEQ_DEV, EXPERTS, TOPK, CAP, 2))(routes_keys, routes_turns).reshape((SEQS, TOPK))
    route_scores = jnp.clip(jnp.exp(math.log(1.0) - 2.306499 * jax.random.uniform(own_keys[15], (SEQS, TOPK), jnp.float32) ** steps_of(own_keys[15], (SEQS, TOPK), ((0, 16),), -0.2, 0.2)), 0.099609375, 1.0).astype(jnp.bfloat16)
    expert_gate = gaussian(splits[16], (EXPERTS, D, FE), D ** -0.5, 0.125, ((0, 16),))
    expert_up = gaussian(splits[17], (EXPERTS, D, FE), D ** -0.5, 0.125, ((0, 16),))
    expert_down = gaussian(splits[18], (EXPERTS, FE, D), FE ** -0.5, 0.25, ((0, 16),))
    dense_gate = gaussian(splits[19], (D, FFD), D ** -0.5, 0.125, ((1, 16),))
    dense_up = gaussian(splits[20], (D, FFD), D ** -0.5, 0.125, ((1, 16),))
    dense_down = gaussian(splits[21], (FFD, D), FFD ** -0.5, 0.0625, ((0, 16),))
    branch_weight = gaussian(splits[22], (D,), D ** -0.5, 0.125)
    return {"resid": resid, "norm_gains": norm_gains, "w_query": w_query, "w_key": w_key, "w_value": w_value, "w_outgate": w_outgate, "w_igate": w_igate, "w_fgate": w_fgate, "igate_bias": igate_bias, "fgate_bias": fgate_bias, "state_matrix": state_matrix, "state_norm": state_norm, "state_max": state_max, "w_mix_out": w_mix_out, "routes": routes, "route_scores": route_scores, "expert_gate": expert_gate, "expert_up": expert_up, "expert_down": expert_down, "dense_gate": dense_gate, "dense_up": dense_up, "dense_down": dense_down, "branch_weight": branch_weight}


def rms_scale(values, gains):
    return values * lax.rsqrt(lax.optimization_barrier(jnp.mean(values * values, axis=-1, keepdims=True)) + 1e-06) * gains.astype(jnp.float32)

def round_half(values):
    return lax.optimization_barrier(values.astype(jnp.bfloat16)).astype(jnp.float32)

def expert_ffn(picked, gate_matrix, up_matrix, down_matrix):
    gate_out = jnp.dot(picked, gate_matrix, preferred_element_type=jnp.float32)
    up_out = jnp.dot(picked, up_matrix, preferred_element_type=jnp.float32)
    hidden = (jax.nn.silu(gate_out) * up_out).astype(jnp.bfloat16)
    return jnp.dot(hidden, down_matrix, preferred_element_type=jnp.float32).astype(jnp.bfloat16)

def expert_mix(branch_in, routes, route_scores, expert_gate, expert_up, expert_down):
    tokens = branch_in.shape[0]
    experts = expert_gate.shape[0]
    onehot = (routes[:, :, None] == jnp.arange(experts, dtype=jnp.int32)[None, None, :]).astype(jnp.float32)
    scores = route_scores.astype(jnp.float32)
    shares = scores / lax.optimization_barrier(jnp.sum(scores, axis=-1, keepdims=True))
    weights = lax.optimization_barrier(jnp.sum(shares[:, :, None] * onehot, axis=1))
    hit_count = lax.optimization_barrier(jnp.sum(onehot, axis=1))
    hit_int = hit_count.astype(jnp.int32).reshape(N_EP, SEQ_DEV, experts)
    rank_index = jnp.cumsum(hit_int, axis=1) - hit_int
    block_base = (jnp.arange(N_EP, dtype=jnp.int32) * CAP)[:, None, None]
    slot_index = (rank_index + block_base).reshape(tokens, experts).T
    hit_flags = hit_count.T
    weight_rows = weights.T
    slot_range = jnp.arange(N_EP * CAP, dtype=jnp.int32)

    def expert_step(running_sum, expert_index):
        chosen = ((slot_index[expert_index][None, :] == slot_range[:, None]) & (hit_flags[expert_index][None, :] > 0.5)).astype(jnp.float32)
        picked = jnp.dot(chosen.astype(jnp.bfloat16), branch_in, preferred_element_type=jnp.float32).astype(jnp.bfloat16)
        produced = expert_ffn(picked, expert_gate[expert_index], expert_up[expert_index], expert_down[expert_index])
        weighted = chosen * weight_rows[expert_index][None, :]
        contribution = jnp.dot(weighted.T, produced.astype(jnp.float32), precision=lax.Precision.HIGHEST)
        running_sum = running_sum + round_half(contribution)
        return (running_sum, None)
    start_sum = jnp.zeros(branch_in.shape, jnp.float32)
    result, ignored = lax.scan(expert_step, start_sum, jnp.arange(experts, dtype=jnp.int32))
    return result

def reference(resid, norm_gains, w_query, w_key, w_value, w_outgate, w_igate, w_fgate, igate_bias, fgate_bias, state_matrix, state_norm, state_max, w_mix_out, routes, route_scores, expert_gate, expert_up, expert_down, dense_gate, dense_up, dense_down, branch_weight):
    seqs = resid.shape[0]
    heads = state_matrix.shape[1]
    head_size = state_matrix.shape[2]
    resid32 = resid.astype(jnp.float32)
    normed = rms_scale(resid32, norm_gains[0]).astype(jnp.bfloat16)

    def project(matrix):
        result = jnp.dot(normed, matrix, preferred_element_type=jnp.float32).astype(jnp.bfloat16)
        return result.astype(jnp.float32).reshape(seqs, heads, head_size)
    query = project(w_query)
    key_heads = project(w_key) * head_size ** (-0.5)
    value_heads = project(w_value)
    outgate = project(w_outgate)
    ipre = jnp.dot(normed, w_igate, preferred_element_type=jnp.float32) + igate_bias
    fpre = jnp.dot(normed, w_fgate, preferred_element_type=jnp.float32) + fgate_bias
    logf = jax.nn.log_sigmoid(fpre)
    new_max = jnp.maximum(ipre, logf + state_max)
    keep_gain = jnp.exp(logf + state_max - new_max)
    write_gain = jnp.exp(ipre - new_max)
    new_matrix = keep_gain[:, :, None, None] * state_matrix + write_gain[:, :, None, None] * value_heads[:, :, :, None] * key_heads[:, :, None, :]
    new_norm = keep_gain[:, :, None] * state_norm + write_gain[:, :, None] * key_heads
    numer = jnp.einsum('shed,shd->she', new_matrix, query, precision=lax.Precision.HIGHEST)
    denom = lax.optimization_barrier(jnp.sum(new_norm * query, axis=-1))
    cell = numer / jnp.maximum(jnp.abs(denom), 1.0)[:, :, None]
    gated = (jax.nn.sigmoid(outgate) * cell).reshape(seqs, heads * head_size).astype(jnp.bfloat16)
    mixed = jnp.dot(gated, w_mix_out, preferred_element_type=jnp.float32)
    middle = resid32 + rms_scale(mixed, norm_gains[1])
    branch_in = rms_scale(middle, norm_gains[2]).astype(jnp.bfloat16)
    moe = expert_mix(branch_in, routes, route_scores, expert_gate, expert_up, expert_down)
    gate_out = jnp.dot(branch_in, dense_gate, preferred_element_type=jnp.float32)
    up_out = jnp.dot(branch_in, dense_up, preferred_element_type=jnp.float32)
    hidden = (jax.nn.silu(gate_out) * up_out).astype(jnp.bfloat16)
    logit = jnp.dot(branch_in, branch_weight, preferred_element_type=jnp.float32)
    branch_gate = jax.nn.sigmoid(logit)[:, None]
    block_width = hidden.shape[1] // N_EP
    hidden_blocks = jnp.transpose(hidden.reshape(seqs, N_EP, block_width), (1, 0, 2))
    down_blocks = dense_down.reshape(N_EP, block_width, dense_down.shape[1])

    def dense_step(running_sum, pieces):
        hidden_block, down_block = pieces
        term = jnp.dot(hidden_block, down_block, preferred_element_type=jnp.float32) * branch_gate
        return (running_sum + round_half(term), None)
    dense, ignored = lax.scan(dense_step, jnp.zeros(middle.shape, jnp.float32), (hidden_blocks, down_blocks))
    combined = moe + dense
    out_stream = (middle + rms_scale(combined, norm_gains[3])).astype(jnp.bfloat16)
    return (out_stream, new_matrix, new_norm, new_max)
```

```python
import functools

import jax
import jax.numpy as jnp
from jax import lax
from jax.experimental import pallas as pl
from jax.experimental.pallas import tpu as pltpu
from jax.sharding import PartitionSpec as P

MESH = pl.DeviceIdType.MESH
F32 = jnp.float32
BF16 = jnp.bfloat16
ROWS = 16
STEP_VMEM = 50 * 2**20
CHUNKS = 4
DMA = pltpu.SemaphoreType.DMA


def rms_scale(values, gains):
    return values * lax.rsqrt(jnp.mean(values * values, axis=-1, keepdims=True) + 1e-06) * gains


def dot_t(left, right):
    return lax.dot_general(left, right, (((1,), (1,)), ((), ())), preferred_element_type=F32)


def dot(left, right):
    return jnp.dot(left, right, preferred_element_type=F32)


def near_first(count):
    return sorted(range(1, count), key=lambda k: (min(k, count - k), k))


def fold(values):
    half = values.shape[1] // 2
    return jnp.concatenate([values[:, :half], values[:, half:]], axis=0)


class Place:
    def __init__(self, n):
        self.n, self.groups = n, n // 4
        self.me = lax.axis_index("ep")
        self.a, self.b, self.c = lax.div(self.me, 4), lax.rem(lax.div(self.me, 2), 2), lax.rem(self.me, 2)

    def index(self, slot):
        rc, rb, ra = slot
        a = lax.rem(self.a + ra, self.groups) if ra else self.a
        b = 1 - self.b if rb else self.b
        c = 1 - self.c if rc else self.c
        return (a * 2 + b) * 2 + c

    def device(self, slot):
        return {"ep": self.index(slot)}

    def slots(self):
        return [(rc, rb, ra) for rc in range(2) for rb in range(2) for ra in range(self.groups)]


def push(src, dst, send_sem, recv_sem, to):
    copy = pltpu.make_async_remote_copy(
        src_ref=src, dst_ref=dst, send_sem=send_sem, recv_sem=recv_sem,
        device_id=to, device_id_type=MESH,
    )
    copy.start()
    return copy


def arrived(dst, sem, to):
    pltpu.make_async_remote_copy(
        src_ref=dst, dst_ref=dst, send_sem=sem, recv_sem=sem, device_id=to, device_id_type=MESH,
    ).wait_recv()


def gather(place, buf, send, recv, begin, work, landed):
    groups = place.groups
    near = near_first(groups)
    sent = []

    def ship(slot, to, sem):
        rc, rb, ra = slot
        tc, tb, ta = to
        there = (rc ^ tc, rb ^ tb, (ra - ta) % groups)
        sent.append(push(buf.at[slot], buf.at[there], send.at[sem], recv.at[there], place.device(to)))

    def wait(slot):
        arrived(buf.at[slot], recv.at[slot], place.device((1, 0, 0)))

    begin()
    for k in sorted(near, key=lambda k: (-min(k, groups - k), k)):
        ship((0, 0, 0), (0, 0, k), (0, k))
    ship((0, 0, 0), (0, 1, 0), (1, 0))
    ship((0, 0, 0), (1, 0, 0), (2, 0))
    work()
    first, second = near, [0] + near
    events = [("a", k) for k in first[:2]]
    rest = [("a", k) for k in first[2:]]
    for k in second:
        events.append(("b", k))
        if rest:
            events.append(rest.pop(0))
    events += rest
    for kind, k in events:
        if kind == "a":
            wait((0, 0, k))
            ship((0, 0, k), (0, 1, 0), (1, k))
            ship((0, 0, k), (1, 0, 0), (2, k))
        else:
            wait((0, 1, k))
            ship((0, 1, k), (1, 0, 0), (3, k))
        work()
    landed(0, 0)
    landed(0, 1)
    for rb in range(2):
        for k in range(groups):
            wait((1, rb, k))
        landed(1, rb)
    for copy in sent:
        copy.wait_send()


def step_kernel(
    n, resid_h, gains_h, wq_h, wk_h, wv_h, wo_h, wi_h, wf_h, bi_h, bf_h, smax_h, snorm_h, state_h, mix_h,
    routes_h, scores_h, eg_h, eu_h, ed_h, dg_h, du_h, dd_h, bw_h,
    fresh, norm_out, max_out, out_ref,
    resid, gains, wp, wi, wf, bi, bf, smax, snorm, routes, scores, bw, mix, eg, eu, dg, du, down,
    rows1, rows2, local, landed, halves, q3, k3, wv3, keep3, numer3, gated, middle, share, everything, hid,
    term, recv1, part1, recv2, part2, recv3, own,
    load_s, load_m, load_w, send1, got1, send2, got2, send_x, recv_x, s1, r1, s2, r2, s3, r3,
):
    place = Place(n)
    groups = place.groups
    near = near_first(groups)
    count, d = resid.shape
    heads, size = norm_out.shape[1], norm_out.shape[2]
    width = wq_h.shape[0]
    experts_local = eg.shape[0]
    y_peer, d_peer = (0, 1, 0), (1, 0, 0)

    barrier = pltpu.get_barrier_semaphore()
    greeted = place.slots()[1:]
    for slot in greeted:
        pl.semaphore_signal(barrier, inc=1, device_id=place.device(slot), device_id_type=MESH)

    def loading(pairs, sems):
        copies = [pltpu.make_async_copy(src, dst, sems.at[i]) for i, (src, dst) in enumerate(pairs)]
        for copy in copies:
            copy.start()
        return copies

    small = loading(
        (
            (resid_h, resid), (gains_h, gains), (wi_h, wi), (wf_h, wf), (bi_h, bi), (bf_h, bf), (smax_h, smax),
            (routes_h, routes), (scores_h, scores), (snorm_h, snorm), (bw_h, bw),
            *[(w, wp.at[i * width : (i + 1) * width]) for i, w in enumerate((wq_h, wk_h, wv_h, wo_h))],
        ),
        load_s,
    )
    states = loading([(state_h.at[s], fresh.at[s]) for s in range(count)], load_m)
    wide_d = dg.shape[1]
    wide_e = eg.shape[2]
    big = loading(
        (
            (mix_h, mix), (dg_h, dg), (du_h, du), (eg_h, eg), (eu_h, eu), (dd_h, down.at[0:wide_d]),
            *[(ed_h.at[e], down.at[wide_d + e * wide_e : wide_d + (e + 1) * wide_e]) for e in range(experts_local)],
        ),
        load_w,
    )
    small[0].wait()
    small[1].wait()
    normed = rms_scale(resid[...].astype(F32), gains[0:1, :])
    rows1[0, 0, 0] = fold(normed).astype(BF16)
    normed = normed.astype(BF16)

    gate = {}

    def column(row):
        eye = lax.broadcasted_iota(jnp.int32, (count, count), 0) == lax.broadcasted_iota(jnp.int32, (count, count), 1)
        return jnp.sum(jnp.where(eye, row, 0.0), axis=-1, keepdims=True)

    def gates():
        for copy in small[2:]:
            copy.wait()
        eye = lax.broadcasted_iota(jnp.int32, (heads, heads), 0) == lax.broadcasted_iota(jnp.int32, (heads, heads), 1)
        bias_i = jnp.sum(jnp.where(eye, bi[...], 0.0), axis=-1, keepdims=True)
        bias_f = jnp.sum(jnp.where(eye, bf[...], 0.0), axis=-1, keepdims=True)
        ipre = dot_t(wi[...], normed) + bias_i
        fpre = dot_t(wf[...], normed) + bias_f
        logf = jnp.minimum(fpre, 0.0) - jnp.log1p(jnp.exp(-jnp.abs(fpre)))
        old_max = logf + smax[...]
        new_max = jnp.maximum(ipre, old_max)
        max_out[...] = new_max
        keep, write = jnp.exp(old_max - new_max), jnp.exp(ipre - new_max)
        gate["keep"] = [column(keep[h : h + 1, :]) for h in range(heads)]
        gate["write"] = [column(write[h : h + 1, :]) for h in range(heads)]
        for h in range(heads):
            keep3[:, h, :] = jnp.broadcast_to(gate["keep"][h], (count, size))

    done = {"halved": 0}

    def halve(upto):
        for s in range(done["halved"], min(upto, count)):
            states[s].wait()

            def body(h, carry, s=s):
                start = pl.multiple_of(h * size, size)
                halves[s, :, pl.ds(start, size)] = fresh[s, h].astype(BF16)
                return carry

            lax.fori_loop(0, heads, body, 0, unroll=True)
        done["halved"] = max(done["halved"], min(upto, count))

    steps = iter([gates] + [functools.partial(halve, k) for k in range(1, count + 1)])

    def work_1():
        for _ in range(2):
            piece = next(steps, None)
            if piece is not None:
                piece()

    gather(
        place, rows1, send1, got1, lambda: pl.semaphore_wait(barrier, len(greeted)), work_1, lambda rc, rb: None
    )

    stacked = rows1[...].reshape(n * 2 * count, d // 2)
    left = dot_t(stacked, wp[:, 0 : d // 2]).reshape(n, 2 * count, 4 * width)
    right = dot_t(stacked, wp[:, d // 2 : d]).reshape(n, 2 * count, 4 * width)
    piece = left[:, 0:count, :] + right[:, count : 2 * count, :]
    code = jnp.concatenate([routes[...].astype(F32), scores[...].astype(F32)], axis=0)
    code = jnp.concatenate([code, jnp.zeros((ROWS - count, 4 * width - count), F32)], axis=1)
    x_sent = []
    for i, slot in enumerate(place.slots()):
        local[i] = jnp.concatenate([piece[i], code], axis=0).astype(BF16)
        if i:
            x_sent.append(
                push(local.at[i], landed.at[place.me], send_x.at[i], recv_x.at[place.me], place.device(slot))
            )
    landed[place.me] = local[0]
    while True:
        todo = next(steps, None)
        if todo is None:
            break
        todo()
    for i, slot in enumerate(place.slots()):
        if i:
            arrived(landed.at[place.index(slot)], recv_x.at[place.index(slot)], place.device(slot))

    per_head = size // width
    numers = []
    head_of = lax.broadcasted_iota(jnp.int32, (heads, heads * size), 1) // size
    own_head = head_of == lax.broadcasted_iota(jnp.int32, (heads, heads * size), 0)

    def cell_rows(m, h):
        parts = [
            landed[h * per_head + p, :, m * width : (m + 1) * width].astype(F32)[0:count] for p in range(per_head)
        ]
        return jnp.concatenate(parts, axis=1)

    queries, denoms, writes = [], [], []
    for h in range(heads):
        q = cell_rows(0, h)
        k = cell_rows(1, h) * size ** (-0.5)
        v = cell_rows(2, h)
        new_norm = gate["keep"][h] * snorm[:, h, :] + gate["write"][h] * k
        norm_out[:, h, :] = new_norm
        denoms.append(jnp.maximum(jnp.abs(jnp.sum(new_norm * q, axis=-1, keepdims=True)), 1.0))
        writes.append(gate["write"][h] * v * jnp.sum(k * q, axis=-1, keepdims=True))
        queries.append(q)
        k3[:, h, :] = k
        wv3[:, h, :] = gate["write"][h] * v
    query = jnp.concatenate(queries, axis=1)
    for s in range(count):
        spread = jnp.where(own_head, query[s : s + 1, :], 0.0).astype(BF16)
        numer3[s] = dot_t(spread, halves[s])
    for h in range(heads):
        numer = gate["keep"][h] * numer3[:, h, :] + writes[h]
        outgate = cell_rows(3, h)
        gated[:, h * size : (h + 1) * size] = (jax.nn.sigmoid(outgate) * (numer / denoms[h])).astype(BF16)
    big[0].wait()
    mixed = dot(gated[...], mix[...])
    stream = resid[...].astype(F32) + rms_scale(mixed, gains[1:2, :])
    middle[...] = stream
    rows2[0, 0, 0] = fold(rms_scale(stream, gains[2:3, :])).astype(BF16)

    def update(s, carry):
        k, kept = k3[s], keep3[s]
        columns = wv3[s].T
        for h in range(heads):
            fresh[s, h] = fresh[s, h] * kept[h : h + 1, :] + columns[:, h : h + 1] * k[h : h + 1, :]
        return carry

    def shares():
        cols = lax.broadcasted_iota(jnp.int32, (count, size), 1)
        eye = lax.broadcasted_iota(jnp.int32, (count, size), 0) == cols
        for j in range(n // 2):
            found = [[] for _ in range(experts_local)]
            for slot in place.slots()[2 * j : 2 * j + 2]:
                codes = landed[place.index(slot), :, 0:size].astype(F32)
                r0, r1 = codes[count : count + 1], codes[count + 1 : count + 2]
                c0, c1 = codes[count + 2 : count + 3], codes[count + 3 : count + 4]
                for e in range(experts_local):
                    mine = (place.me * experts_local + e).astype(F32)
                    part = (jnp.where(r0 == mine, c0, 0.0) + jnp.where(r1 == mine, c1, 0.0)) / (c0 + c1)
                    found[e].append(jnp.sum(jnp.where(eye, part, 0.0), axis=-1, keepdims=True))
            for e in range(experts_local):
                value = jnp.concatenate(found[e], axis=0)
                share[e, 2 * j * count : 2 * (j + 1) * count, :] = jnp.broadcast_to(value, (2 * count, size))

    pieces = len(near) * 2 + 2
    cuts = [round(count * i / (pieces - 1)) for i in range(pieces)]
    jobs = iter(
        [functools.partial(lax.fori_loop, cuts[i], cuts[i + 1], update, 0) for i in range(pieces - 1)] + [shares]
    )

    def work_2():
        job = next(jobs, None)
        if job is not None:
            job()

    def unfold(rc, rb):
        base = (rc * 2 + rb) * groups
        for j in range(groups // 2):
            low = rows2[rc, rb, 2 * j].astype(F32)
            high = rows2[rc, rb, 2 * j + 1].astype(F32)
            at = (base + 2 * j) * count
            everything[at : at + 2 * count, 0 : d // 2] = jnp.concatenate(
                [low[0:count], high[0:count]], axis=0
            ).astype(BF16)
            everything[at : at + 2 * count, d // 2 : d] = jnp.concatenate(
                [low[count:], high[count:]], axis=0
            ).astype(BF16)

    gather(place, rows2, send2, got2, lambda: None, work_2, unfold)
    for job in jobs:
        job()

    logit = jnp.zeros((n * count, size), F32)
    for j in range(d // size):
        logit = logit + everything[:, j * size : (j + 1) * size].astype(F32) * bw[j : j + 1, :].astype(F32)
    branch_gate = jax.nn.sigmoid(jnp.sum(logit, axis=-1, keepdims=True))
    for copy in big[1:]:
        copy.wait()

    def ffn(gate_w, up_w, start, scale):
        wide = gate_w.shape[1]
        cut = min(256, wide)
        for j in range(wide // cut):
            cols = slice(j * cut, (j + 1) * cut)
            g = dot(everything[...], gate_w[:, cols])
            u = dot(everything[...], up_w[:, cols])
            hid[:, start + j * cut : start + (j + 1) * cut] = (jax.nn.silu(g) * u * scale).astype(BF16)

    ffn(dg, du, 0, branch_gate)
    for e in range(experts_local):
        ffn(eg.at[e], eu.at[e], wide_d + e * wide_e, share[e, :, 0:1])

    wide = d // CHUNKS
    half, quarter = n * count // 2, n * count // 4
    copies = []
    for h in range(CHUNKS):
        term[h] = dot(hid[...], down[:, h * wide : (h + 1) * wide]).astype(BF16)
        copies.append(push(term.at[h, half : 2 * half], recv1.at[h], s1.at[h], r1.at[h], place.device(d_peer)))
    for h in range(CHUNKS):
        copies[h].wait_recv()
        part1[h] = (term[h, 0:half].astype(F32) + recv1[h].astype(F32)).astype(BF16)
        copies.append(push(part1.at[h, quarter : 2 * quarter], recv2.at[h], s2.at[h], r2.at[h], place.device(y_peer)))
    far = sorted(near, key=lambda k: (-min(k, groups - k), k))
    for h in range(CHUNKS):
        copies[CHUNKS + h].wait_recv()
        value = part1[h, 0:quarter].astype(F32) + recv2[h].astype(F32)
        for k in far:
            part2[h, k] = fold(value[k * count : (k + 1) * count]).astype(BF16)
            there = (groups - k) % groups
            copies.append(
                push(part2.at[h, k], recv3.at[h, there], s3.at[h, k], r3.at[h, there], place.device((0, 0, k)))
            )
        own[h] = fold(value[0:count])
    square = 0.0
    for h in range(CHUNKS):
        value = own[h]
        for k in near:
            arrived(recv3.at[h, k], r3.at[h, k], place.device((0, 0, k)))
            value = value + recv3[h, k].astype(F32)
        own[h] = value
        square = square + jnp.sum(value * value, axis=-1, keepdims=True)
    scale = lax.rsqrt((square[0:count] + square[count:]) / d + 1e-06)
    for h in range(CHUNKS):
        value = own[h]
        for part in range(2):
            cols = slice(h * wide + part * wide // 2, h * wide + (part + 1) * wide // 2)
            extra = value[part * count : (part + 1) * count] * scale * gains[3:4, cols]
            out_ref[:, cols] = (middle[:, cols] + extra).astype(BF16)
    for copy in x_sent + copies:
        copy.wait_send()


def finish_kernel(fresh, norm, top, out, fresh_o, norm_o, top_o, out_o, sems):
    count = fresh.shape[0]
    pairs = [(out, out_o), (norm, norm_o), (top, top_o)] + [(fresh.at[s], fresh_o.at[s]) for s in range(count)]
    copies = [pltpu.make_async_copy(src, dst, sems.at[i]) for i, (src, dst) in enumerate(pairs)]
    for copy in copies:
        copy.start()
    for copy in copies:
        copy.wait()


def local(
    resid, norm_gains, w_query, w_key, w_value, w_outgate, w_igate, w_fgate,
    igate_bias, fgate_bias, state_matrix, state_norm, state_max, w_mix_out,
    routes, route_scores, expert_gate, expert_up, expert_down,
    dense_gate, dense_up, dense_down, branch_weight,
):
    n = lax.axis_size("ep")
    groups = n // 4
    count, d = resid.shape
    _, heads, size, _ = state_matrix.shape
    width = w_query.shape[1]
    experts = expert_gate.shape[0]
    hidden = dense_gate.shape[1] + experts * expert_gate.shape[2]
    wide = d // CHUNKS
    half, quarter = n * count // 2, n * count // 4
    args = [
        resid, norm_gains, w_query.T, w_key.T, w_value.T, w_outgate.T, w_igate.T, w_fgate.T,
        igate_bias[None], fgate_bias[None], state_max.T, state_norm, state_matrix, w_mix_out,
        routes.T, route_scores.T, expert_gate, expert_up, expert_down, dense_gate, dense_up, dense_down,
        branch_weight.reshape(d // size, size),
    ]
    args = [pltpu.with_memory_space_constraint(x, pltpu.HBM) for x in args]
    vmem = pl.BlockSpec(memory_space=pltpu.VMEM)
    hbm = pl.BlockSpec(memory_space=pltpu.HBM)
    kept = (
        pltpu.VMEM(state_matrix.shape, F32),
        pltpu.VMEM(state_norm.shape, F32),
        pltpu.VMEM((heads, count), F32),
        pltpu.VMEM((count, d), BF16),
    )
    small = pltpu.VMEM((count, heads, size), F32)
    results = pl.pallas_call(
        functools.partial(step_kernel, n),
        out_shape=kept,
        in_specs=[hbm] * len(args),
        out_specs=(vmem,) * 4,
        scratch_shapes=[
            pltpu.VMEM((count, d), BF16),
            pltpu.VMEM(norm_gains.shape, F32),
            pltpu.VMEM((4 * width, d), BF16),
            pltpu.VMEM((heads, d), BF16),
            pltpu.VMEM((heads, d), BF16),
            pltpu.VMEM((1, heads), F32),
            pltpu.VMEM((1, heads), F32),
            pltpu.VMEM((heads, count), F32),
            pltpu.VMEM(state_norm.shape, F32),
            pltpu.VMEM((routes.shape[1], count), jnp.int32),
            pltpu.VMEM((routes.shape[1], count), BF16),
            pltpu.VMEM((d // size, size), BF16),
            pltpu.VMEM(w_mix_out.shape, BF16),
            pltpu.VMEM(expert_gate.shape, BF16),
            pltpu.VMEM(expert_up.shape, BF16),
            pltpu.VMEM(dense_gate.shape, BF16),
            pltpu.VMEM(dense_up.shape, BF16),
            pltpu.VMEM((hidden, d), BF16),
            pltpu.VMEM((2, 2, groups, 2 * count, d // 2), BF16),
            pltpu.VMEM((2, 2, groups, 2 * count, d // 2), BF16),
            pltpu.VMEM((n, ROWS, 4 * width), BF16),
            pltpu.VMEM((n, ROWS, 4 * width), BF16),
            pltpu.VMEM((count, size, heads * size), BF16),
            small, small, small, small, small,
            pltpu.VMEM((count, heads * size), BF16),
            pltpu.VMEM((count, d), F32),
            pltpu.VMEM((experts, n * count, size), F32),
            pltpu.VMEM((n * count, d), BF16),
            pltpu.VMEM((n * count, hidden), BF16),
            pltpu.VMEM((CHUNKS, 2 * half, wide), BF16),
            pltpu.VMEM((CHUNKS, half, wide), BF16),
            pltpu.VMEM((CHUNKS, half, wide), BF16),
            pltpu.VMEM((CHUNKS, quarter, wide), BF16),
            pltpu.VMEM((CHUNKS, groups, 2 * count, wide // 2), BF16),
            pltpu.VMEM((CHUNKS, groups, 2 * count, wide // 2), BF16),
            pltpu.VMEM((CHUNKS, 2 * count, wide // 2), F32),
            DMA((15,)),
            DMA((count,)),
            DMA((6 + experts,)),
            DMA((4, groups)),
            DMA((2, 2, groups)),
            DMA((4, groups)),
            DMA((2, 2, groups)),
            DMA((n,)),
            DMA((n,)),
            DMA((CHUNKS,)),
            DMA((CHUNKS,)),
            DMA((CHUNKS,)),
            DMA((CHUNKS,)),
            DMA((CHUNKS, groups)),
            DMA((CHUNKS, groups)),
        ],
        compiler_params=pltpu.CompilerParams(
            collective_id=0, has_side_effects=True, vmem_limit_bytes=STEP_VMEM
        ),
        name="step",
    )(*args)
    new_matrix, new_norm, new_max, out_stream = pl.pallas_call(
        finish_kernel,
        out_shape=(
            jax.ShapeDtypeStruct(state_matrix.shape, F32),
            jax.ShapeDtypeStruct(state_norm.shape, F32),
            jax.ShapeDtypeStruct((heads, count), F32),
            jax.ShapeDtypeStruct((count, d), BF16),
        ),
        in_specs=[vmem] * 4,
        out_specs=(hbm,) * 4,
        scratch_shapes=[DMA((3 + count,))],
        name="finish",
    )(*results)
    return (out_stream, new_matrix, new_norm, new_max.T)


def solution(mesh):
    rows = ("grp", "ep")
    placed = (
        P(rows, None),
        P(),
        P(None, "ep"),
        P(None, "ep"),
        P(None, "ep"),
        P(None, "ep"),
        P(),
        P(),
        P(),
        P(),
        P(rows, None, None, None),
        P(rows, None, None),
        P(rows, None),
        P(),
        P(rows, None),
        P(rows, None),
        P("ep", None, None),
        P("ep", None, None),
        P("ep", None, None),
        P(None, "ep"),
        P(None, "ep"),
        P("ep", None),
        P(),
    )
    return jax.shard_map(
        local,
        mesh=mesh,
        in_specs=placed,
        out_specs=(
            P(rows, None),
            P(rows, None, None, None),
            P(rows, None, None),
            P(rows, None),
        ),
        check_vma=False,
    )
```

```python
import functools

import jax
import jax.numpy as jnp
from jax import lax
from jax.experimental import pallas as pl
from jax.experimental.pallas import tpu as pltpu
from jax.sharding import PartitionSpec as P

MESH = pl.DeviceIdType.MESH
F32 = jnp.float32
BF16 = jnp.bfloat16
ROWS = 16
STEP_VMEM = 50 * 2**20
CHUNKS = 4
DMA = pltpu.SemaphoreType.DMA


def rms_scale(values, gains):
    return values * lax.rsqrt(jnp.mean(values * values, axis=-1, keepdims=True) + 1e-06) * gains


def dot_t(left, right):
    return lax.dot_general(left, right, (((1,), (1,)), ((), ())), preferred_element_type=F32)


def dot(left, right):
    return jnp.dot(left, right, preferred_element_type=F32)


def fold(values):
    half = values.shape[1] // 2
    return jnp.concatenate([values[:, :half], values[:, half:]], axis=0)


class Place:
    def __init__(self, n):
        self.n, self.groups = n, n // 4
        self.me = lax.axis_index("ep")
        self.a, self.b, self.c = lax.div(self.me, 4), lax.rem(lax.div(self.me, 2), 2), lax.rem(self.me, 2)
        self.near = [self.ranked(i) for i in range(self.groups - 1)]

    def ranked(self, i):
        ahead = 0
        for a in range(self.groups):
            others = sorted((k for k in range(self.groups) if k != a), key=lambda k: (abs(k - a), k))
            ahead = jnp.where(self.a == a, (others[i] - a) % self.groups, ahead)
        return ahead

    def back(self, ra):
        return lax.rem(self.groups - ra, self.groups)

    def index(self, slot):
        rc, rb, ra = slot
        a = self.a if isinstance(ra, int) and ra == 0 else lax.rem(self.a + ra, self.groups)
        b = 1 - self.b if rb else self.b
        c = 1 - self.c if rc else self.c
        return (a * 2 + b) * 2 + c

    def device(self, slot):
        return {"ep": self.index(slot)}

    def slots(self):
        return [(rc, rb, ra) for rb in range(2) for rc in range(2) for ra in range(self.groups)]


def push(src, dst, send_sem, recv_sem, to):
    copy = pltpu.make_async_remote_copy(
        src_ref=src, dst_ref=dst, send_sem=send_sem, recv_sem=recv_sem,
        device_id=to, device_id_type=MESH,
    )
    copy.start()
    return copy


def arrived(dst, sem, to):
    pltpu.make_async_remote_copy(
        src_ref=dst, dst_ref=dst, send_sem=sem, recv_sem=sem, device_id=to, device_id_type=MESH,
    ).wait_recv()


def gather(place, buf, send, recv, work, tag):
    groups, near = place.groups, place.near
    a_dirs, b_dir, c_dir = near, (0, 1, 0), (1, 0, 0)
    sent = []

    def ship(slot, half, there, to):
        block, far = buf.at[(*slot, half)], (*there, half)
        sent.append(push(block, buf.at[far], send.at[len(sent)], recv.at[far], place.device(to)))

    def along(rb, half, order):
        for ra in order:
            ship((0, rb, 0), half, (0, rb, place.back(ra)), (0, 0, ra))

    def across(slot, half, to):
        rc, rb, ra = slot
        ship(slot, half, (rc ^ to[0], rb ^ to[1], ra), to)

    def wait(slot, half):
        arrived(buf.at[(*slot, half)], recv.at[(*slot, half)], place.device(c_dir))

    across((0, 0, 0), 1, b_dir)
    along(0, 0, near[::-1])
    along(0, 1, near[::-1])
    across((0, 0, 0), 0, b_dir)
    across((0, 0, 0), 0, c_dir)
    across((0, 0, 0), 1, c_dir)
    work("sent")

    def own_side(i, half):
        slot = (0, 0, near[i])
        wait(slot, half)
        if half == 0:
            across(slot, half, b_dir)
        across(slot, half, c_dir)

    def other_side(slot, half, own=False):
        wait(slot, half)
        if own and half == 1:
            along(1, 1, near)
        across(slot, half, c_dir)

    last = groups - 2
    other_side((0, 1, 0), 1, own=True)
    own_side(0, 0)
    other_side((0, 1, 0), 0)
    for i in range(1, groups):
        if i <= last:
            own_side(i, 0)
        own_side(i - 1, 1)
    work("sides")
    for ra in range(groups):
        for half in range(2):
            wait((1, 0, ra), half)
    work("near")
    for i in range(groups - 1):
        for half in (1, 0):
            other_side((0, 1, near[i]), half)
        work("far")
    work("relayed")
    for ra in range(groups):
        for half in range(2):
            wait((1, 1, ra), half)
    work("done")
    for copy in sent:
        copy.wait_send()


def step_kernel(
    n, resid_h, gains_h, wq_h, wk_h, wv_h, wo_h, wi_h, wf_h, bi_h, bf_h, smax_h, snorm_h, state_h, mix_h,
    routes_h, scores_h, eg_h, eu_h, ed_h, dg_h, du_h, dd_h, bw_h,
    fresh, norm_out, max_out, out_ref,
    resid, gains, wp, wi, wf, bi, bf, smax, snorm, routes, scores, bw, mix, eg, eu, dg, du, down,
    rows1, rows2, local, landed, halves, krow, wv3, keep3, numer3, gated, middle, share, everything, hid,
    term, recv1, part_z, recv_z, own_z, part_zy, recv_zy, part_y, recv_y, own_y, part_yz, recv_yz,
    load_s, load_m, load_w, send1, got1, send2, got2, send_x, recv_x, s1, r1, s2, r2, s3, r3, s_y, r_y,
):
    place = Place(n)
    groups = place.groups
    near = place.near
    count, d = resid.shape
    heads, size = norm_out.shape[1], norm_out.shape[2]
    width = wq_h.shape[0]
    experts_local = eg.shape[0]
    b_dir, c_dir = (0, 1, 0), (1, 0, 0)

    barrier = pltpu.get_barrier_semaphore()
    greeted = place.slots()[1:]
    for slot in greeted:
        pl.semaphore_signal(barrier, inc=1, device_id=place.device(slot), device_id_type=MESH)

    def loading(pairs, sems):
        copies = [pltpu.make_async_copy(src, dst, sems.at[i]) for i, (src, dst) in enumerate(pairs)]
        for copy in copies:
            copy.start()
        return copies

    small = loading(
        (
            (resid_h, resid), (gains_h, gains), (wi_h, wi), (wf_h, wf), (bi_h, bi), (bf_h, bf), (smax_h, smax),
            (routes_h, routes), (scores_h, scores), (snorm_h, snorm), (bw_h, bw),
            *[(w, wp.at[i * width : (i + 1) * width]) for i, w in enumerate((wq_h, wk_h, wv_h, wo_h))],
        ),
        load_s,
    )
    wide_d, wide_e = dg.shape[1], eg.shape[2]
    states, big = [], []

    def load_rest():
        states.extend(loading([(state_h.at[s], fresh.at[s]) for s in range(count)], load_m))
        big.extend(
            loading(
                (
                    (mix_h, mix), (dg_h, dg), (du_h, du), (eg_h, eg), (eu_h, eu), (dd_h, down.at[0:wide_d]),
                    *[
                        (ed_h.at[e], down.at[wide_d + e * wide_e : wide_d + (e + 1) * wide_e])
                        for e in range(experts_local)
                    ],
                ),
                load_w,
            )
        )

    small[0].wait()
    small[1].wait()
    normed = rms_scale(resid[...].astype(F32), gains[0:1, :])
    for half in range(2):
        rows1[0, 0, 0, half] = fold(normed[:, half * d // 2 : (half + 1) * d // 2]).astype(BF16)
    normed = normed.astype(BF16)

    gate = {}

    def column(row):
        eye = lax.broadcasted_iota(jnp.int32, (count, count), 0) == lax.broadcasted_iota(jnp.int32, (count, count), 1)
        return jnp.sum(jnp.where(eye, row, 0.0), axis=-1, keepdims=True)

    def gates():
        for copy in small[2:]:
            copy.wait()
        eye = lax.broadcasted_iota(jnp.int32, (heads, heads), 0) == lax.broadcasted_iota(jnp.int32, (heads, heads), 1)
        bias_i = jnp.sum(jnp.where(eye, bi[...], 0.0), axis=-1, keepdims=True)
        bias_f = jnp.sum(jnp.where(eye, bf[...], 0.0), axis=-1, keepdims=True)
        ipre = dot_t(wi[...], normed) + bias_i
        fpre = dot_t(wf[...], normed) + bias_f
        logf = jnp.minimum(fpre, 0.0) - jnp.log1p(jnp.exp(-jnp.abs(fpre)))
        old_max = logf + smax[...]
        new_max = jnp.maximum(ipre, old_max)
        max_out[...] = new_max
        keep, write = jnp.exp(old_max - new_max), jnp.exp(ipre - new_max)
        gate["keep"] = [column(keep[h : h + 1, :]) for h in range(heads)]
        gate["write"] = [column(write[h : h + 1, :]) for h in range(heads)]
        for h in range(heads):
            keep3[:, h, :] = jnp.broadcast_to(gate["keep"][h], (count, size))

    def halve(upto):
        for s in range(upto):
            states[s].wait()

            def body(h, carry, s=s):
                start = pl.multiple_of(h * size, size)
                halves[s, :, pl.ds(start, size)] = fresh[s, h].astype(BF16)
                return carry

            lax.fori_loop(0, heads, body, 0, unroll=True)
    def work_1(point):
        if point == "sent":
            gates()
            load_rest()

    pl.semaphore_wait(barrier, len(greeted))
    gather(place, rows1, send1, got1, work_1, "g1")

    piece = 0.0
    for half in range(2):
        stacked = rows1[:, :, :, half].reshape(n * 2 * count, d // 4)
        for part in range(2):
            q = (2 * half + part) * d // 4
            value = dot_t(stacked, wp[:, q : q + d // 4]).reshape(n, 2 * count, 4 * width)
            piece = piece + value[:, part * count : (part + 1) * count, :]
    code = jnp.concatenate([routes[...].astype(F32), scores[...].astype(F32)], axis=0)
    code = jnp.concatenate([code, jnp.zeros((ROWS - count, 4 * width - count), F32)], axis=1)
    x_sent = []
    for i, slot in enumerate(place.slots()):
        rc, rb, ra = slot
        local[i] = jnp.concatenate([piece[(rc * 2 + rb) * groups + ra], code], axis=0).astype(BF16)
        if i:
            x_sent.append(
                push(local.at[i], landed.at[place.me], send_x.at[i], recv_x.at[place.me], place.device(slot))
            )
    landed[place.me] = local[0]
    halve(count)
    for i, slot in enumerate(place.slots()):
        if i:
            arrived(landed.at[place.index(slot)], recv_x.at[place.index(slot)], place.device(slot))

    per_head = size // width
    numers = []
    head_of = lax.broadcasted_iota(jnp.int32, (heads, heads * size), 1) // size
    own_head = head_of == lax.broadcasted_iota(jnp.int32, (heads, heads * size), 0)

    def cell_rows(m, h):
        parts = [
            landed[h * per_head + p, :, m * width : (m + 1) * width].astype(F32)[0:count] for p in range(per_head)
        ]
        return jnp.concatenate(parts, axis=1)

    queries, keys, denoms, writes = [], [], [], []
    for h in range(heads):
        q = cell_rows(0, h)
        raw = cell_rows(1, h)
        k = raw * size ** (-0.5)
        v = cell_rows(2, h)
        new_norm = gate["keep"][h] * snorm[:, h, :] + gate["write"][h] * k
        norm_out[:, h, :] = new_norm
        denoms.append(jnp.maximum(jnp.abs(jnp.sum(new_norm * q, axis=-1, keepdims=True)), 1.0))
        writes.append(gate["write"][h] * v * jnp.sum(k * q, axis=-1, keepdims=True))
        queries.append(q)
        wv3[:, h, :] = gate["write"][h] * v * size ** (-0.5)
        keys.append(raw)
    query = jnp.concatenate(queries, axis=1)
    key_rows = jnp.concatenate(keys, axis=1)
    for s in range(count):
        krow[s] = key_rows[s : s + 1, :]
    for s in range(count):
        spread = jnp.where(own_head, query[s : s + 1, :], 0.0).astype(BF16)
        numer3[s] = dot_t(spread, halves[s])
    for h in range(heads):
        numer = gate["keep"][h] * numer3[:, h, :] + writes[h]
        outgate = cell_rows(3, h)
        gated[:, h * size : (h + 1) * size] = (jax.nn.sigmoid(outgate) * (numer / denoms[h])).astype(BF16)
    big[0].wait()
    mixed = dot(gated[...], mix[...])
    stream = resid[...].astype(F32) + rms_scale(mixed, gains[1:2, :])
    middle[...] = stream
    branch_in = rms_scale(stream, gains[2:3, :])
    for half in range(2):
        rows2[0, 0, 0, half] = fold(branch_in[:, half * d // 2 : (half + 1) * d // 2]).astype(BF16)

    def update(s, carry):
        value = wv3[s]
        parts = []
        for _ in range(3):
            parts.append(value.astype(BF16))
            value = value - parts[-1].astype(F32)
        key = jnp.where(own_head, krow[s], 0.0).astype(BF16)
        outer = lax.dot_general(
            jnp.concatenate(parts, axis=0), jnp.concatenate([key] * 3, axis=0),
            (((0,), (0,)), ((), ())), preferred_element_type=F32,
        )
        kept = keep3[s]
        for h in range(heads):
            fresh[s, h] = fresh[s, h] * kept[h : h + 1, :] + outer[:, h * size : (h + 1) * size]
        return carry

    def shares():
        cols = lax.broadcasted_iota(jnp.int32, (count, size), 1)
        eye = lax.broadcasted_iota(jnp.int32, (count, size), 0) == cols
        for j in range(n // 2):
            found = [[] for _ in range(experts_local)]
            for slot in place.slots()[2 * j : 2 * j + 2]:
                codes = landed[place.index(slot), :, 0:size].astype(F32)
                r0, r1 = codes[count : count + 1], codes[count + 1 : count + 2]
                c0, c1 = codes[count + 2 : count + 3], codes[count + 3 : count + 4]
                for e in range(experts_local):
                    mine = (place.me * experts_local + e).astype(F32)
                    part = (jnp.where(r0 == mine, c0, 0.0) + jnp.where(r1 == mine, c1, 0.0)) / (c0 + c1)
                    found[e].append(jnp.sum(jnp.where(eye, part, 0.0), axis=-1, keepdims=True))
            for e in range(experts_local):
                value = jnp.concatenate(found[e], axis=0)
                share[e, 2 * j * count : 2 * (j + 1) * count, :] = jnp.broadcast_to(value, (2 * count, size))

    updated = {"at": 0}

    def updates(upto):
        upto = round(count * upto)
        lax.fori_loop(updated["at"], upto, update, 0, unroll=True)
        updated["at"] = upto

    rows_half = n * count // 2

    def unfold(rb):
        for rc in range(2):
            base = (rb * 2 + rc) * groups
            for j in range(groups // 2):
                at = (base + 2 * j) * count
                for half in range(2):
                    pair = [rows2[rc, rb, 2 * j + i, half].astype(F32) for i in range(2)]
                    for part in range(2):
                        q = (2 * half + part) * d // 4
                        everything[at : at + 2 * count, q : q + d // 4] = jnp.concatenate(
                            [value[part * count : (part + 1) * count] for value in pair], axis=0
                        ).astype(BF16)

    def ups(rb):
        rows = slice(rb * rows_half, (rb + 1) * rows_half)
        logit = jnp.zeros((rows_half, size), F32)
        for j in range(d // size):
            logit = logit + everything[rows, j * size : (j + 1) * size].astype(F32) * bw[j : j + 1, :].astype(F32)
        branch_gate = jax.nn.sigmoid(jnp.sum(logit, axis=-1, keepdims=True))
        parts = [(dg, du, 0, branch_gate)]
        parts += [(eg.at[e], eu.at[e], wide_d + e * wide_e, share[e, rows, 0:1]) for e in range(experts_local)]
        for gate_w, up_w, start, scale in parts:
            wide = gate_w.shape[1]
            cut = min(256, wide)
            for j in range(wide // cut):
                cols = slice(j * cut, (j + 1) * cut)
                g = dot(everything[rows, :], gate_w[:, cols])
                u = dot(everything[rows, :], up_w[:, cols])
                hid[rows, start + j * cut : start + (j + 1) * cut] = (jax.nn.silu(g) * u * scale).astype(BF16)
                yield

    todo = {}

    def some(rb, count):
        for _ in range(count):
            next(todo[rb], None)

    def work_2(point):
        if point == "sent":
            updates(0.25)
            shares()
        elif point == "near":
            unfold(0)
            for copy in big[1:5]:
                copy.wait()
            todo[0] = ups(0)
        elif point == "far":
            some(0, 1)
        elif point == "relayed":
            some(0, 99)
        elif point == "done":
            unfold(1)
            todo[1] = ups(1)

    gather(place, rows2, send2, got2, work_2, "g2")

    some(1, 99)
    for copy in big[5:]:
        copy.wait()

    wide, quarter, piece = d // 2, n * count // 4, d // CHUNKS
    each = CHUNKS // 2
    downs, copies = {}, []

    def down_proj(h):
        value = dot(hid[...], down[:, h * piece : (h + 1) * piece]).astype(BF16)
        cols = slice(h % each * piece, (h % each + 1) * piece)
        term[h // each, :, :, cols] = value.reshape(2, 2 * quarter, piece)
        downs[h] = push(
            term.at[h // each, :, quarter : 2 * quarter, cols], recv1.at[h // each, :, :, cols],
            s1.at[h], r1.at[h], place.device(c_dir),
        )

    def sum_c(g):
        for h in range(g * each, (g + 1) * each):
            downs[h].wait_recv()
        return term[g, :, 0:quarter].astype(F32) + recv1[g].astype(F32)

    def along(parts, lands, sems):
        for i, ra in enumerate(near[::-1]):
            there = place.back(ra)
            copies.append(
                push(parts.at[ra], lands.at[there], sems[0].at[i], sems[1].at[there], place.device((0, 0, ra)))
            )

    def landed_a(value, lands, sem):
        for ra in near:
            arrived(lands.at[ra], sem.at[ra], place.device((0, 0, ra)))
        for ra in range(1, groups):
            value = value + lands[ra].astype(F32)
        return value

    for h in range(each + 1):
        down_proj(h)
    value = sum_c(0)
    for ra in range(groups):
        both = jnp.concatenate([value[rb, ra * count : (ra + 1) * count] for rb in range(2)], axis=0)
        if ra:
            part_z[ra] = both.astype(BF16)
        else:
            own_z[...] = both
    along(part_z, recv_z, (s2, r2))
    for h in range(each + 1, 2 * each):
        down_proj(h)
    value = sum_c(1)
    part_y[...] = value[1].astype(BF16)
    own_y[...] = value[0]
    swap_y = push(part_y, recv_y, s_y.at[0], r_y.at[0], place.device(b_dir))
    updates(0.7)
    swap_y.wait_recv()
    value = own_y[...] + recv_y[...].astype(F32)
    for ra in range(1, groups):
        part_yz[ra] = fold(value[ra * count : (ra + 1) * count]).astype(BF16)
    along(part_yz, recv_yz, (s3, r3))
    finals = [None, fold(value[0:count])]
    value = landed_a(own_z[...], recv_z, r2)
    part_zy[...] = fold(value[count:]).astype(BF16)
    finals[0] = fold(value[0:count])
    swap_z = push(part_zy, recv_zy, s_y.at[1], r_y.at[1], place.device(b_dir))
    updates(1)
    finals[1] = landed_a(finals[1], recv_yz, r3)
    swap_z.wait_recv()
    finals[0] = finals[0] + recv_zy[...].astype(F32)
    square = sum(jnp.sum(value * value, axis=-1, keepdims=True) for value in finals)
    scale = lax.rsqrt((square[0:count] + square[count:]) / d + 1e-06)
    for g in range(2):
        for part in range(2):
            cols = slice(g * wide + part * wide // 2, g * wide + (part + 1) * wide // 2)
            extra = finals[g][part * count : (part + 1) * count] * scale * gains[3:4, cols]
            out_ref[:, cols] = (middle[:, cols] + extra).astype(BF16)
    for copy in x_sent + list(downs.values()) + [swap_y, swap_z] + copies:
        copy.wait_send()


def finish_kernel(fresh, norm, top, out, fresh_o, norm_o, top_o, out_o, sems):
    count = fresh.shape[0]
    pairs = [(out, out_o), (norm, norm_o), (top, top_o)] + [(fresh.at[s], fresh_o.at[s]) for s in range(count)]
    copies = [pltpu.make_async_copy(src, dst, sems.at[i]) for i, (src, dst) in enumerate(pairs)]
    for copy in copies:
        copy.start()
    for copy in copies:
        copy.wait()


def local(
    resid, norm_gains, w_query, w_key, w_value, w_outgate, w_igate, w_fgate,
    igate_bias, fgate_bias, state_matrix, state_norm, state_max, w_mix_out,
    routes, route_scores, expert_gate, expert_up, expert_down,
    dense_gate, dense_up, dense_down, branch_weight,
):
    n = lax.axis_size("ep")
    groups = n // 4
    count, d = resid.shape
    _, heads, size, _ = state_matrix.shape
    width = w_query.shape[1]
    experts = expert_gate.shape[0]
    hidden = dense_gate.shape[1] + experts * expert_gate.shape[2]
    wide = d // 2
    quarter = n * count // 4
    args = [
        resid, norm_gains, w_query.T, w_key.T, w_value.T, w_outgate.T, w_igate.T, w_fgate.T,
        igate_bias[None], fgate_bias[None], state_max.T, state_norm, state_matrix, w_mix_out,
        routes.T, route_scores.T, expert_gate, expert_up, expert_down, dense_gate, dense_up, dense_down,
        branch_weight.reshape(d // size, size),
    ]
    args = [pltpu.with_memory_space_constraint(x, pltpu.HBM) for x in args]
    vmem = pl.BlockSpec(memory_space=pltpu.VMEM)
    hbm = pl.BlockSpec(memory_space=pltpu.HBM)
    kept = (
        pltpu.VMEM(state_matrix.shape, F32),
        pltpu.VMEM(state_norm.shape, F32),
        pltpu.VMEM((heads, count), F32),
        pltpu.VMEM((count, d), BF16),
    )
    small = pltpu.VMEM((count, heads, size), F32)
    results = pl.pallas_call(
        functools.partial(step_kernel, n),
        out_shape=kept,
        in_specs=[hbm] * len(args),
        out_specs=(vmem,) * 4,
        scratch_shapes=[
            pltpu.VMEM((count, d), BF16),
            pltpu.VMEM(norm_gains.shape, F32),
            pltpu.VMEM((4 * width, d), BF16),
            pltpu.VMEM((heads, d), BF16),
            pltpu.VMEM((heads, d), BF16),
            pltpu.VMEM((1, heads), F32),
            pltpu.VMEM((1, heads), F32),
            pltpu.VMEM((heads, count), F32),
            pltpu.VMEM(state_norm.shape, F32),
            pltpu.VMEM((routes.shape[1], count), jnp.int32),
            pltpu.VMEM((routes.shape[1], count), BF16),
            pltpu.VMEM((d // size, size), BF16),
            pltpu.VMEM(w_mix_out.shape, BF16),
            pltpu.VMEM(expert_gate.shape, BF16),
            pltpu.VMEM(expert_up.shape, BF16),
            pltpu.VMEM(dense_gate.shape, BF16),
            pltpu.VMEM(dense_up.shape, BF16),
            pltpu.VMEM((hidden, d), BF16),
            pltpu.VMEM((2, 2, groups, 2, 2 * count, d // 4), BF16),
            pltpu.VMEM((2, 2, groups, 2, 2 * count, d // 4), BF16),
            pltpu.VMEM((n, ROWS, 4 * width), BF16),
            pltpu.VMEM((n, ROWS, 4 * width), BF16),
            pltpu.VMEM((count, size, heads * size), BF16),
            pltpu.VMEM((count, 1, heads * size), F32),
            small, small, small,
            pltpu.VMEM((count, heads * size), BF16),
            pltpu.VMEM((count, d), F32),
            pltpu.VMEM((experts, n * count, size), F32),
            pltpu.VMEM((n * count, d), BF16),
            pltpu.VMEM((n * count, hidden), BF16),
            pltpu.VMEM((2, 2, 2 * quarter, wide), BF16),
            pltpu.VMEM((2, 2, quarter, wide), BF16),
            pltpu.VMEM((groups, 2 * count, wide), BF16),
            pltpu.VMEM((groups, 2 * count, wide), BF16),
            pltpu.VMEM((2 * count, wide), F32),
            pltpu.VMEM((2 * count, wide // 2), BF16),
            pltpu.VMEM((2 * count, wide // 2), BF16),
            pltpu.VMEM((quarter, wide), BF16),
            pltpu.VMEM((quarter, wide), BF16),
            pltpu.VMEM((quarter, wide), F32),
            pltpu.VMEM((groups, 2 * count, wide // 2), BF16),
            pltpu.VMEM((groups, 2 * count, wide // 2), BF16),
            DMA((15,)),
            DMA((count,)),
            DMA((6 + experts,)),
            DMA((10 * groups,)),
            DMA((2, 2, groups, 2)),
            DMA((10 * groups,)),
            DMA((2, 2, groups, 2)),
            DMA((n,)),
            DMA((n,)),
            DMA((CHUNKS,)),
            DMA((CHUNKS,)),
            DMA((groups,)),
            DMA((groups,)),
            DMA((groups,)),
            DMA((groups,)),
            DMA((2,)),
            DMA((2,)),
        ],
        compiler_params=pltpu.CompilerParams(
            collective_id=0, has_side_effects=True, vmem_limit_bytes=STEP_VMEM
        ),
        name="step",
    )(*args)
    new_matrix, new_norm, new_max, out_stream = pl.pallas_call(
        finish_kernel,
        out_shape=(
            jax.ShapeDtypeStruct(state_matrix.shape, F32),
            jax.ShapeDtypeStruct(state_norm.shape, F32),
            jax.ShapeDtypeStruct((heads, count), F32),
            jax.ShapeDtypeStruct((count, d), BF16),
        ),
        in_specs=[vmem] * 4,
        out_specs=(hbm,) * 4,
        scratch_shapes=[DMA((3 + count,))],
        compiler_params=pltpu.CompilerParams(vmem_limit_bytes=2**20),
        name="finish",
    )(*results)
    return (out_stream, new_matrix, new_norm, new_max.T)


def solution(mesh):
    rows = ("grp", "ep")
    placed = (
        P(rows, None),
        P(),
        P(None, "ep"),
        P(None, "ep"),
        P(None, "ep"),
        P(None, "ep"),
        P(),
        P(),
        P(),
        P(),
        P(rows, None, None, None),
        P(rows, None, None),
        P(rows, None),
        P(),
        P(rows, None),
        P(rows, None),
        P("ep", None, None),
        P("ep", None, None),
        P("ep", None, None),
        P(None, "ep"),
        P(None, "ep"),
        P("ep", None),
        P(),
    )
    return jax.shard_map(
        local,
        mesh=mesh,
        in_specs=placed,
        out_specs=(
            P(rows, None),
            P(rows, None, None, None),
            P(rows, None, None),
            P(rows, None),
        ),
        check_vma=False,
    )
```

```python
import functools

import jax
import jax.numpy as jnp
from jax import lax
from jax.experimental import pallas as pl
from jax.experimental.pallas import tpu as pltpu
from jax.sharding import PartitionSpec as P

MESH = pl.DeviceIdType.MESH
F32 = jnp.float32
BF16 = jnp.bfloat16
ROWS = 16
STEP_VMEM = 50 * 2**20
CHUNKS = 4
HALVE_AT = {"first": 0.25, "second": 0.5, "third": 1}
PROJECT_AT = {"sides": (0, 0), "near": (1, 0), "relayed": (0, 1), "done": (1, 1)}
DMA = pltpu.SemaphoreType.DMA


def rms_scale(values, gains):
    return values * lax.rsqrt(jnp.mean(values * values, axis=-1, keepdims=True) + 1e-06) * gains


def dot_t(left, right):
    return lax.dot_general(left, right, (((1,), (1,)), ((), ())), preferred_element_type=F32)


def dot(left, right):
    return jnp.dot(left, right, preferred_element_type=F32)


def fold(values):
    half = values.shape[1] // 2
    return jnp.concatenate([values[:, :half], values[:, half:]], axis=0)


class Place:
    def __init__(self, n):
        self.n, self.groups = n, n // 4
        self.me = lax.axis_index("ep")
        self.a, self.b, self.c = lax.div(self.me, 4), lax.rem(lax.div(self.me, 2), 2), lax.rem(self.me, 2)
        far = self.groups - 1
        self.near = [self.ranked(i, lambda k, a: (abs(k - a), -abs(2 * k - far))) for i in range(far)]
        self.first = [self.ranked(i, lambda k, a: k) for i in range(self.groups - 1)]

    def ranked(self, i, rank):
        ahead = 0
        for a in range(self.groups):
            others = sorted((k for k in range(self.groups) if k != a), key=lambda k: (rank(k, a), k))
            ahead = jnp.where(self.a == a, (others[i] - a) % self.groups, ahead)
        return ahead

    def back(self, ra):
        return lax.rem(self.groups - ra, self.groups)

    def index(self, slot):
        rc, rb, ra = slot
        a = self.a if isinstance(ra, int) and ra == 0 else lax.rem(self.a + ra, self.groups)
        b = 1 - self.b if rb else self.b
        c = 1 - self.c if rc else self.c
        return (a * 2 + b) * 2 + c

    def device(self, slot):
        return {"ep": self.index(slot)}

    def slots(self):
        return [(rc, rb, ra) for rb in range(2) for rc in range(2) for ra in range(self.groups)]


def push(src, dst, send_sem, recv_sem, to):
    copy = pltpu.make_async_remote_copy(
        src_ref=src, dst_ref=dst, send_sem=send_sem, recv_sem=recv_sem,
        device_id=to, device_id_type=MESH,
    )
    copy.start()
    return copy


def arrived(dst, sem, to):
    pltpu.make_async_remote_copy(
        src_ref=dst, dst_ref=dst, send_sem=sem, recv_sem=sem, device_id=to, device_id_type=MESH,
    ).wait_recv()


def gather(place, buf, send, recv, work, tag):
    groups, near = place.groups, place.near
    a_dirs, b_dir, c_dir = near, (0, 1, 0), (1, 0, 0)
    sent = []

    def ship(slot, half, there, to):
        block, far = buf.at[(*slot, half)], (*there, half)
        sent.append(push(block, buf.at[far], send.at[len(sent)], recv.at[far], place.device(to)))

    def along(rb, half, order):
        for ra in order:
            ship((0, rb, 0), half, (0, rb, place.back(ra)), (0, 0, ra))

    def across(slot, half, to):
        rc, rb, ra = slot
        ship(slot, half, (rc ^ to[0], rb ^ to[1], ra), to)

    def wait(slot, half):
        arrived(buf.at[(*slot, half)], recv.at[(*slot, half)], place.device(c_dir))

    across((0, 0, 0), 1, b_dir)
    along(0, 0, near[::-1])
    along(0, 1, near[::-1])
    across((0, 0, 0), 0, b_dir)
    across((0, 0, 0), 0, c_dir)
    across((0, 0, 0), 1, c_dir)
    work("sent")

    def own_side(i, half):
        slot = (0, 0, near[i])
        wait(slot, half)
        if half == 0:
            across(slot, half, b_dir)
        across(slot, half, c_dir)

    def other_side(slot, half, own=False):
        wait(slot, half)
        if own and half == 1:
            along(1, 1, near)
        across(slot, half, c_dir)

    last = groups - 2
    other_side((0, 1, 0), 1, own=True)
    own_side(0, 0)
    other_side((0, 1, 0), 0)
    work("first")
    for i in range(1, groups):
        if i <= last:
            own_side(i, 0)
        own_side(i - 1, 1)
        if i < groups - 1:
            work("second" if i == 1 else "third")
    work("sides")
    for ra in range(groups):
        for half in range(2):
            wait((1, 0, ra), half)
    work("near")
    for i in range(groups - 1):
        for half in (1, 0):
            other_side((0, 1, near[i]), half)
        work("far")
    work("relayed")
    for ra in range(groups):
        for half in range(2):
            wait((1, 1, ra), half)
    work("done")
    for copy in sent:
        copy.wait_send()


def step_kernel(
    n, resid_h, gains_h, wq_h, wk_h, wv_h, wo_h, wi_h, wf_h, bi_h, bf_h, smax_h, snorm_h, state_h, mix_h,
    routes_h, scores_h, eg_h, eu_h, ed_h, dg_h, du_h, dd_h, bw_h,
    fresh, norm_out, max_out, out_ref,
    resid, gains, wp, wi, wf, bi, bf, smax, snorm, routes, scores, bw, mix, eg, eu, dg, du, down,
    rows1, rows2, local, landed, halves, krow, wv3, keep3, numer3, gated, middle, share, everything, hid,
    term, recv1, part_z, recv_z, own_z, part_zy, recv_zy, part_y, recv_y, own_y, part_yz, recv_yz,
    load_s, load_m, load_w, send1, got1, send2, got2, send_x, recv_x, s1, r1, s2, r2, s3, r3, s_y, r_y,
):
    place = Place(n)
    groups = place.groups
    near = place.near
    count, d = resid.shape
    heads, size = norm_out.shape[1], norm_out.shape[2]
    width = wq_h.shape[0]
    experts_local = eg.shape[0]
    b_dir, c_dir = (0, 1, 0), (1, 0, 0)

    barrier = pltpu.get_barrier_semaphore()
    greeted = place.slots()[1:]
    for slot in greeted:
        pl.semaphore_signal(barrier, inc=1, device_id=place.device(slot), device_id_type=MESH)

    def loading(pairs, sems):
        copies = [pltpu.make_async_copy(src, dst, sems.at[i]) for i, (src, dst) in enumerate(pairs)]
        for copy in copies:
            copy.start()
        return copies

    small = loading(
        (
            (resid_h, resid), (gains_h, gains), (wi_h, wi), (wf_h, wf), (bi_h, bi), (bf_h, bf), (smax_h, smax),
            (routes_h, routes), (scores_h, scores), (snorm_h, snorm), (bw_h, bw),
            *[(w, wp.at[i * width : (i + 1) * width]) for i, w in enumerate((wq_h, wk_h, wv_h, wo_h))],
        ),
        load_s,
    )
    wide_d, wide_e = dg.shape[1], eg.shape[2]
    states, big = [], []

    def load_rest():
        states.extend(loading([(state_h.at[s], fresh.at[s]) for s in range(count)], load_m))
        big.extend(
            loading(
                (
                    (mix_h, mix), (dg_h, dg), (du_h, du), (eg_h, eg), (eu_h, eu), (dd_h, down.at[0:wide_d]),
                    *[
                        (ed_h.at[e], down.at[wide_d + e * wide_e : wide_d + (e + 1) * wide_e])
                        for e in range(experts_local)
                    ],
                ),
                load_w,
            )
        )

    small[0].wait()
    small[1].wait()
    normed = rms_scale(resid[...].astype(F32), gains[0:1, :])
    for half in range(2):
        rows1[0, 0, 0, half] = fold(normed[:, half * d // 2 : (half + 1) * d // 2]).astype(BF16)
    normed = normed.astype(BF16)

    gate = {}

    def column(row):
        eye = lax.broadcasted_iota(jnp.int32, (count, count), 0) == lax.broadcasted_iota(jnp.int32, (count, count), 1)
        return jnp.sum(jnp.where(eye, row, 0.0), axis=-1, keepdims=True)

    def gates():
        for copy in small[2:]:
            copy.wait()
        eye = lax.broadcasted_iota(jnp.int32, (heads, heads), 0) == lax.broadcasted_iota(jnp.int32, (heads, heads), 1)
        bias_i = jnp.sum(jnp.where(eye, bi[...], 0.0), axis=-1, keepdims=True)
        bias_f = jnp.sum(jnp.where(eye, bf[...], 0.0), axis=-1, keepdims=True)
        ipre = dot_t(wi[...], normed) + bias_i
        fpre = dot_t(wf[...], normed) + bias_f
        logf = jnp.minimum(fpre, 0.0) - jnp.log1p(jnp.exp(-jnp.abs(fpre)))
        old_max = logf + smax[...]
        new_max = jnp.maximum(ipre, old_max)
        max_out[...] = new_max
        keep, write = jnp.exp(old_max - new_max), jnp.exp(ipre - new_max)
        gate["keep"] = [column(keep[h : h + 1, :]) for h in range(heads)]
        gate["write"] = [column(write[h : h + 1, :]) for h in range(heads)]
        for h in range(heads):
            keep3[:, h, :] = jnp.broadcast_to(gate["keep"][h], (count, size))

    halved = {"at": 0}

    def halve(upto):
        for s in range(halved["at"], upto):
            states[s].wait()
            for h in range(heads):
                halves[s, h * size : (h + 1) * size, :] = fresh[s, h].astype(BF16).T
        halved["at"] = upto

    x_sent = []

    def project(rc, rb):
        piece = 0.0
        for half in range(2):
            stacked = rows1[rc, rb, :, half].reshape(groups * 2 * count, d // 4)
            for part in range(2):
                q = (2 * half + part) * d // 4
                value = dot_t(stacked, wp[:, q : q + d // 4]).reshape(groups, 2 * count, 4 * width)
                piece = piece + value[:, part * count : (part + 1) * count, :]
        code = jnp.concatenate([routes[...].astype(F32), scores[...].astype(F32)], axis=0)
        code = jnp.concatenate([code, jnp.zeros((ROWS - count, 4 * width - count), F32)], axis=1)
        for ra in range(groups):
            slot = (rc, rb, ra)
            i = (rc * 2 + rb) * groups + ra
            local[i] = jnp.concatenate([piece[ra], code], axis=0).astype(BF16)
            if i:
                x_sent.append(
                    push(local.at[i], landed.at[place.me], send_x.at[i], recv_x.at[place.me], place.device(slot))
                )
            else:
                landed[place.me] = local[0]

    def work_1(point):
        if point == "sent":
            gates()
            load_rest()
        elif point in HALVE_AT:
            halve(round(count * HALVE_AT[point]))
        elif point in PROJECT_AT:
            project(*PROJECT_AT[point])

    pl.semaphore_wait(barrier, len(greeted))
    gather(place, rows1, send1, got1, work_1, "g1")

    halve(count)
    for i, slot in enumerate(place.slots()):
        if i:
            arrived(landed.at[place.index(slot)], recv_x.at[place.index(slot)], place.device(slot))

    per_head = size // width
    numers = []
    head_of = lax.broadcasted_iota(jnp.int32, (heads, heads * size), 1) // size
    own_head = head_of == lax.broadcasted_iota(jnp.int32, (heads, heads * size), 0)

    def cell_rows(m, h):
        parts = [
            landed[h * per_head + p, :, m * width : (m + 1) * width].astype(F32)[0:count] for p in range(per_head)
        ]
        return jnp.concatenate(parts, axis=1)

    queries, keys, denoms, writes = [], [], [], []
    for h in range(heads):
        q = cell_rows(0, h)
        raw = cell_rows(1, h)
        k = raw * size ** (-0.5)
        v = cell_rows(2, h)
        new_norm = gate["keep"][h] * snorm[:, h, :] + gate["write"][h] * k
        norm_out[:, h, :] = new_norm
        denoms.append(jnp.maximum(jnp.abs(jnp.sum(new_norm * q, axis=-1, keepdims=True)), 1.0))
        writes.append(gate["write"][h] * v * jnp.sum(k * q, axis=-1, keepdims=True))
        queries.append(q)
        wv3[:, h, :] = gate["write"][h] * v * size ** (-0.5)
        keys.append(raw)
    query = jnp.concatenate(queries, axis=1)
    key_rows = jnp.concatenate(keys, axis=1)
    for s in range(count):
        krow[s] = key_rows[s : s + 1, :]
    for s in range(count):
        spread = jnp.where(own_head, query[s : s + 1, :], 0.0).astype(BF16)
        numer3[s] = dot(spread, halves[s])
    for h in range(heads):
        numer = gate["keep"][h] * numer3[:, h, :] + writes[h]
        outgate = cell_rows(3, h)
        gated[:, h * size : (h + 1) * size] = (jax.nn.sigmoid(outgate) * (numer / denoms[h])).astype(BF16)
    big[0].wait()
    mixed = dot(gated[...], mix[...])
    stream = resid[...].astype(F32) + rms_scale(mixed, gains[1:2, :])
    middle[...] = stream
    branch_in = rms_scale(stream, gains[2:3, :])
    for half in range(2):
        rows2[0, 0, 0, half] = fold(branch_in[:, half * d // 2 : (half + 1) * d // 2]).astype(BF16)

    def update(s, carry):
        value = wv3[s]
        parts = []
        for _ in range(3):
            parts.append(value.astype(BF16))
            value = value - parts[-1].astype(F32)
        key = jnp.where(own_head, krow[s], 0.0).astype(BF16)
        outer = lax.dot_general(
            jnp.concatenate(parts, axis=0), jnp.concatenate([key] * 3, axis=0),
            (((0,), (0,)), ((), ())), preferred_element_type=F32,
        )
        kept = keep3[s]
        for h in range(heads):
            fresh[s, h] = fresh[s, h] * kept[h : h + 1, :] + outer[:, h * size : (h + 1) * size]
        return carry

    def shares():
        cols = lax.broadcasted_iota(jnp.int32, (count, size), 1)
        eye = lax.broadcasted_iota(jnp.int32, (count, size), 0) == cols
        for j in range(n // 2):
            found = [[] for _ in range(experts_local)]
            for slot in place.slots()[2 * j : 2 * j + 2]:
                codes = landed[place.index(slot), :, 0:size].astype(F32)
                r0, r1 = codes[count : count + 1], codes[count + 1 : count + 2]
                c0, c1 = codes[count + 2 : count + 3], codes[count + 3 : count + 4]
                for e in range(experts_local):
                    mine = (place.me * experts_local + e).astype(F32)
                    part = (jnp.where(r0 == mine, c0, 0.0) + jnp.where(r1 == mine, c1, 0.0)) / (c0 + c1)
                    found[e].append(jnp.sum(jnp.where(eye, part, 0.0), axis=-1, keepdims=True))
            for e in range(experts_local):
                value = jnp.concatenate(found[e], axis=0)
                share[e, 2 * j * count : 2 * (j + 1) * count, :] = jnp.broadcast_to(value, (2 * count, size))

    updated = {"at": 0}

    def updates(upto):
        upto = round(count * upto)
        lax.fori_loop(updated["at"], upto, update, 0, unroll=True)
        updated["at"] = upto

    rows_half = n * count // 2

    def unfold(rb):
        for rc in range(2):
            base = (rb * 2 + rc) * groups
            for j in range(groups // 2):
                at = (base + 2 * j) * count
                for half in range(2):
                    pair = [rows2[rc, rb, 2 * j + i, half].astype(F32) for i in range(2)]
                    for part in range(2):
                        q = (2 * half + part) * d // 4
                        everything[at : at + 2 * count, q : q + d // 4] = jnp.concatenate(
                            [value[part * count : (part + 1) * count] for value in pair], axis=0
                        ).astype(BF16)

    def ups(rb):
        rows = slice(rb * rows_half, (rb + 1) * rows_half)
        logit = jnp.zeros((rows_half, size), F32)
        for j in range(d // size):
            logit = logit + everything[rows, j * size : (j + 1) * size].astype(F32) * bw[j : j + 1, :].astype(F32)
        branch_gate = jax.nn.sigmoid(jnp.sum(logit, axis=-1, keepdims=True))
        parts = [(dg, du, 0, branch_gate)]
        parts += [(eg.at[e], eu.at[e], wide_d + e * wide_e, share[e, rows, 0:1]) for e in range(experts_local)]
        for gate_w, up_w, start, scale in parts:
            wide = gate_w.shape[1]
            cut = min(256, wide)
            for j in range(wide // cut):
                cols = slice(j * cut, (j + 1) * cut)
                g = dot(everything[rows, :], gate_w[:, cols])
                u = dot(everything[rows, :], up_w[:, cols])
                hid[rows, start + j * cut : start + (j + 1) * cut] = (jax.nn.silu(g) * u * scale).astype(BF16)
                yield

    todo = {}

    def some(rb, count):
        for _ in range(count):
            next(todo[rb], None)

    wide, quarter = d // 2, n * count // 4
    downs, copies = {}, []

    def down_proj(rb):
        for copy in big[5:] if rb == 0 else []:
            copy.wait()
        for g in range(2):
            rows = slice(rb * rows_half, (rb + 1) * rows_half)
            term[g, rb] = dot(hid[rows, :], down[:, g * wide : (g + 1) * wide]).astype(BF16)
            downs[g, rb] = push(
                term.at[g, rb, quarter : 2 * quarter], recv1.at[g, rb], s1.at[2 * rb + g], r1.at[2 * rb + g],
                place.device(c_dir),
            )

    def work_2(point):
        if point == "sent":
            updates(0.25)
            shares()
        elif point == "near":
            unfold(0)
            for copy in big[1:5]:
                copy.wait()
            todo[0] = ups(0)
        elif point == "far":
            some(0, 1)
        elif point == "relayed":
            some(0, 99)
            down_proj(0)
        elif point == "done":
            unfold(1)
            todo[1] = ups(1)

    gather(place, rows2, send2, got2, work_2, "g2")

    some(1, 99)
    down_proj(1)

    def sum_c(g, rb):
        downs[g, rb].wait_recv()
        return term[g, rb, 0:quarter].astype(F32) + recv1[g, rb].astype(F32)

    def along(parts, lands, sems):
        for i, ra in enumerate(place.first):
            there = place.back(ra)
            copies.append(
                push(parts.at[ra], lands.at[there], sems[0].at[i], sems[1].at[there], place.device((0, 0, ra)))
            )

    def landed_a(value, lands, sem):
        for ra in near:
            arrived(lands.at[ra], sem.at[ra], place.device((0, 0, ra)))
        for ra in range(1, groups):
            value = value + lands[ra].astype(F32)
        return value

    value = [sum_c(0, rb) for rb in range(2)]
    for ra in range(groups):
        both = jnp.concatenate([value[rb][ra * count : (ra + 1) * count] for rb in range(2)], axis=0)
        if ra:
            part_z[ra] = both.astype(BF16)
        else:
            own_z[...] = both
    along(part_z, recv_z, (s2, r2))
    part_y[...] = sum_c(1, 1).astype(BF16)
    own_y[...] = sum_c(1, 0)
    swap_y = push(part_y, recv_y, s_y.at[0], r_y.at[0], place.device(b_dir))
    updates(0.7)
    swap_y.wait_recv()
    value = own_y[...] + recv_y[...].astype(F32)
    for ra in range(1, groups):
        part_yz[ra] = fold(value[ra * count : (ra + 1) * count]).astype(BF16)
    along(part_yz, recv_yz, (s3, r3))
    finals = [None, fold(value[0:count])]
    value = landed_a(own_z[...], recv_z, r2)
    part_zy[...] = fold(value[count:]).astype(BF16)
    finals[0] = fold(value[0:count])
    swap_z = push(part_zy, recv_zy, s_y.at[1], r_y.at[1], place.device(b_dir))
    updates(1)
    finals[1] = landed_a(finals[1], recv_yz, r3)
    swap_z.wait_recv()
    finals[0] = finals[0] + recv_zy[...].astype(F32)
    square = sum(jnp.sum(value * value, axis=-1, keepdims=True) for value in finals)
    scale = lax.rsqrt((square[0:count] + square[count:]) / d + 1e-06)
    for g in range(2):
        for part in range(2):
            cols = slice(g * wide + part * wide // 2, g * wide + (part + 1) * wide // 2)
            extra = finals[g][part * count : (part + 1) * count] * scale * gains[3:4, cols]
            out_ref[:, cols] = (middle[:, cols] + extra).astype(BF16)
    for copy in x_sent + list(downs.values()) + [swap_y, swap_z] + copies:
        copy.wait_send()


def finish_kernel(fresh, norm, top, out, fresh_o, norm_o, top_o, out_o, sems):
    count = fresh.shape[0]
    pairs = [(out, out_o), (norm, norm_o), (top, top_o)] + [(fresh.at[s], fresh_o.at[s]) for s in range(count)]
    copies = [pltpu.make_async_copy(src, dst, sems.at[i]) for i, (src, dst) in enumerate(pairs)]
    for copy in copies:
        copy.start()
    for copy in copies:
        copy.wait()


def local(
    resid, norm_gains, w_query, w_key, w_value, w_outgate, w_igate, w_fgate,
    igate_bias, fgate_bias, state_matrix, state_norm, state_max, w_mix_out,
    routes, route_scores, expert_gate, expert_up, expert_down,
    dense_gate, dense_up, dense_down, branch_weight,
):
    n = lax.axis_size("ep")
    groups = n // 4
    count, d = resid.shape
    _, heads, size, _ = state_matrix.shape
    width = w_query.shape[1]
    experts = expert_gate.shape[0]
    hidden = dense_gate.shape[1] + experts * expert_gate.shape[2]
    wide = d // 2
    quarter = n * count // 4
    args = [
        resid, norm_gains, w_query.T, w_key.T, w_value.T, w_outgate.T, w_igate.T, w_fgate.T,
        igate_bias[None], fgate_bias[None], state_max.T, state_norm, state_matrix, w_mix_out,
        routes.T, route_scores.T, expert_gate, expert_up, expert_down, dense_gate, dense_up, dense_down,
        branch_weight.reshape(d // size, size),
    ]
    args = [pltpu.with_memory_space_constraint(x, pltpu.HBM) for x in args]
    vmem = pl.BlockSpec(memory_space=pltpu.VMEM)
    hbm = pl.BlockSpec(memory_space=pltpu.HBM)
    kept = (
        pltpu.VMEM(state_matrix.shape, F32),
        pltpu.VMEM(state_norm.shape, F32),
        pltpu.VMEM((heads, count), F32),
        pltpu.VMEM((count, d), BF16),
    )
    small = pltpu.VMEM((count, heads, size), F32)
    results = pl.pallas_call(
        functools.partial(step_kernel, n),
        out_shape=kept,
        in_specs=[hbm] * len(args),
        out_specs=(vmem,) * 4,
        scratch_shapes=[
            pltpu.VMEM((count, d), BF16),
            pltpu.VMEM(norm_gains.shape, F32),
            pltpu.VMEM((4 * width, d), BF16),
            pltpu.VMEM((heads, d), BF16),
            pltpu.VMEM((heads, d), BF16),
            pltpu.VMEM((1, heads), F32),
            pltpu.VMEM((1, heads), F32),
            pltpu.VMEM((heads, count), F32),
            pltpu.VMEM(state_norm.shape, F32),
            pltpu.VMEM((routes.shape[1], count), jnp.int32),
            pltpu.VMEM((routes.shape[1], count), BF16),
            pltpu.VMEM((d // size, size), BF16),
            pltpu.VMEM(w_mix_out.shape, BF16),
            pltpu.VMEM(expert_gate.shape, BF16),
            pltpu.VMEM(expert_up.shape, BF16),
            pltpu.VMEM(dense_gate.shape, BF16),
            pltpu.VMEM(dense_up.shape, BF16),
            pltpu.VMEM((hidden, d), BF16),
            pltpu.VMEM((2, 2, groups, 2, 2 * count, d // 4), BF16),
            pltpu.VMEM((2, 2, groups, 2, 2 * count, d // 4), BF16),
            pltpu.VMEM((n, ROWS, 4 * width), BF16),
            pltpu.VMEM((n, ROWS, 4 * width), BF16),
            pltpu.VMEM((count, heads * size, size), BF16),
            pltpu.VMEM((count, 1, heads * size), F32),
            small, small, small,
            pltpu.VMEM((count, heads * size), BF16),
            pltpu.VMEM((count, d), F32),
            pltpu.VMEM((experts, n * count, size), F32),
            pltpu.VMEM((n * count, d), BF16),
            pltpu.VMEM((n * count, hidden), BF16),
            pltpu.VMEM((2, 2, 2 * quarter, wide), BF16),
            pltpu.VMEM((2, 2, quarter, wide), BF16),
            pltpu.VMEM((groups, 2 * count, wide), BF16),
            pltpu.VMEM((groups, 2 * count, wide), BF16),
            pltpu.VMEM((2 * count, wide), F32),
            pltpu.VMEM((2 * count, wide // 2), BF16),
            pltpu.VMEM((2 * count, wide // 2), BF16),
            pltpu.VMEM((quarter, wide), BF16),
            pltpu.VMEM((quarter, wide), BF16),
            pltpu.VMEM((quarter, wide), F32),
            pltpu.VMEM((groups, 2 * count, wide // 2), BF16),
            pltpu.VMEM((groups, 2 * count, wide // 2), BF16),
            DMA((15,)),
            DMA((count,)),
            DMA((6 + experts,)),
            DMA((10 * groups,)),
            DMA((2, 2, groups, 2)),
            DMA((10 * groups,)),
            DMA((2, 2, groups, 2)),
            DMA((n,)),
            DMA((n,)),
            DMA((CHUNKS,)),
            DMA((CHUNKS,)),
            DMA((groups,)),
            DMA((groups,)),
            DMA((groups,)),
            DMA((groups,)),
            DMA((2,)),
            DMA((2,)),
        ],
        compiler_params=pltpu.CompilerParams(
            collective_id=0, has_side_effects=True, vmem_limit_bytes=STEP_VMEM
        ),
        name="step",
    )(*args)
    new_matrix, new_norm, new_max, out_stream = pl.pallas_call(
        finish_kernel,
        out_shape=(
            jax.ShapeDtypeStruct(state_matrix.shape, F32),
            jax.ShapeDtypeStruct(state_norm.shape, F32),
            jax.ShapeDtypeStruct((heads, count), F32),
            jax.ShapeDtypeStruct((count, d), BF16),
        ),
        in_specs=[vmem] * 4,
        out_specs=(hbm,) * 4,
        scratch_shapes=[DMA((3 + count,))],
        compiler_params=pltpu.CompilerParams(vmem_limit_bytes=2**20),
        name="finish",
    )(*results)
    return (out_stream, new_matrix, new_norm, new_max.T)


def solution(mesh):
    rows = ("grp", "ep")
    placed = (
        P(rows, None),
        P(),
        P(None, "ep"),
        P(None, "ep"),
        P(None, "ep"),
        P(None, "ep"),
        P(),
        P(),
        P(),
        P(),
        P(rows, None, None, None),
        P(rows, None, None),
        P(rows, None),
        P(),
        P(rows, None),
        P(rows, None),
        P("ep", None, None),
        P("ep", None, None),
        P("ep", None, None),
        P(None, "ep"),
        P(None, "ep"),
        P("ep", None),
        P(),
    )
    return jax.shard_map(
        local,
        mesh=mesh,
        in_specs=placed,
        out_specs=(
            P(rows, None),
            P(rows, None, None, None),
            P(rows, None, None),
            P(rows, None),
        ),
        check_vma=False,
    )
```

```python
import functools
import itertools

import jax
import jax.numpy as jnp
from jax import lax
from jax.experimental import pallas as pl
from jax.experimental.pallas import tpu as pltpu
from jax.sharding import PartitionSpec as P

MESH = pl.DeviceIdType.MESH
F32 = jnp.float32
BF16 = jnp.bfloat16
ROWS = 16
STEP_VMEM = 50 * 2**20
CHUNKS = 4
PIECE = 256
AHEAD = 3
HALVE_AT = {"first": 0.25, "second": 0.25, "third": 0.5}
PROJECT_AT = {"sides": (0, 0), "near": (1, 0), "relayed": (0, 1), "done": (1, 1)}
DMA = pltpu.SemaphoreType.DMA


def rms_scale(values, gains):
    return values * lax.rsqrt(jnp.mean(values * values, axis=-1, keepdims=True) + 1e-06) * gains


def dot_t(left, right):
    return lax.dot_general(left, right, (((1,), (1,)), ((), ())), preferred_element_type=F32)


def dot(left, right):
    return jnp.dot(left, right, preferred_element_type=F32)


def fold(values):
    half = values.shape[1] // 2
    return jnp.concatenate([values[:, :half], values[:, half:]], axis=0)


class Place:
    def __init__(self, n):
        self.n, self.groups = n, n // 4
        self.me = lax.axis_index("ep")
        self.a, self.b, self.c = lax.div(self.me, 4), lax.rem(lax.div(self.me, 2), 2), lax.rem(self.me, 2)
        far = self.groups - 1
        self.near = [self.ranked(i, lambda k, a: (abs(k - a), -abs(2 * k - far))) for i in range(far)]
        self.first = [self.ranked(i, lambda k, a: k) for i in range(self.groups - 1)]

    def ranked(self, i, rank):
        ahead = 0
        for a in range(self.groups):
            others = sorted((k for k in range(self.groups) if k != a), key=lambda k: (rank(k, a), k))
            ahead = jnp.where(self.a == a, (others[i] - a) % self.groups, ahead)
        return ahead

    def back(self, ra):
        return lax.rem(self.groups - ra, self.groups)

    def index(self, slot):
        rc, rb, ra = slot
        a = self.a if isinstance(ra, int) and ra == 0 else lax.rem(self.a + ra, self.groups)
        b = 1 - self.b if rb else self.b
        c = 1 - self.c if rc else self.c
        return (a * 2 + b) * 2 + c

    def device(self, slot):
        return {"ep": self.index(slot)}

    def slots(self):
        return [(rc, rb, ra) for rb in range(2) for rc in range(2) for ra in range(self.groups)]


def push(src, dst, send_sem, recv_sem, to):
    copy = pltpu.make_async_remote_copy(
        src_ref=src, dst_ref=dst, send_sem=send_sem, recv_sem=recv_sem,
        device_id=to, device_id_type=MESH,
    )
    copy.start()
    return copy


def arrived(dst, sem, to):
    pltpu.make_async_remote_copy(
        src_ref=dst, dst_ref=dst, send_sem=sem, recv_sem=sem, device_id=to, device_id_type=MESH,
    ).wait_recv()


def gather(place, buf, send, recv, work, tag):
    groups, near = place.groups, place.near
    a_dirs, b_dir, c_dir = near, (0, 1, 0), (1, 0, 0)
    sent = []

    def ship(slot, half, there, to):
        block, far = buf.at[(*slot, half)], (*there, half)
        sent.append(push(block, buf.at[far], send.at[len(sent)], recv.at[far], place.device(to)))

    def along(rb, half, order):
        for ra in order:
            ship((0, rb, 0), half, (0, rb, place.back(ra)), (0, 0, ra))

    def across(slot, half, to):
        rc, rb, ra = slot
        ship(slot, half, (rc ^ to[0], rb ^ to[1], ra), to)

    def wait(slot, half):
        arrived(buf.at[(*slot, half)], recv.at[(*slot, half)], place.device(c_dir))

    across((0, 0, 0), 1, b_dir)
    along(0, 0, near[::-1])
    along(0, 1, near[::-1])
    across((0, 0, 0), 0, b_dir)
    across((0, 0, 0), 0, c_dir)
    across((0, 0, 0), 1, c_dir)
    work("sent")

    def own_side(i, half):
        slot = (0, 0, near[i])
        wait(slot, half)
        if half == 0:
            across(slot, half, b_dir)
        across(slot, half, c_dir)

    def other_side(slot, half, own=False):
        wait(slot, half)
        if own and half == 1:
            along(1, 1, near)
        across(slot, half, c_dir)

    last = groups - 2
    other_side((0, 1, 0), 1, own=True)
    own_side(0, 0)
    other_side((0, 1, 0), 0)
    work("first")
    for i in range(1, groups):
        if i <= last:
            own_side(i, 0)
        own_side(i - 1, 1)
        if i < groups - 1:
            work("second" if i == 1 else "third")
    work("sides")
    for ra in range(groups):
        for half in range(2):
            wait((1, 0, ra), half)
    work("near")
    for i in range(groups - 1):
        for half in (1, 0):
            other_side((0, 1, near[i]), half)
        work("far")
    work("relayed")
    for ra in range(groups):
        for half in range(2):
            wait((1, 1, ra), half)
    work("done")
    for copy in sent:
        copy.wait_send()


def step_kernel(
    n, resid_h, gains_h, wq_h, wk_h, wv_h, wo_h, wi_h, wf_h, bi_h, bf_h, smax_h, snorm_h, state_h, mix_h,
    routes_h, scores_h, eg_h, eu_h, ed_h, dg_h, du_h, dd_h, bw_h,
    fresh, norm_out, max_out, out_ref,
    resid, gains, wp, wi, wf, bi, bf, smax, snorm, routes, scores, bw, mix, eg, eu, dg, du, down,
    rows1, rows2, local, landed, halves, krow, wv3, keep3, numer3, gated, middle, share, everything, hid,
    term, recv1, part_z, recv_z, own_z, part_zy, recv_zy, part_y, recv_y, own_y, part_yz, recv_yz,
    load_s, load_m, load_w, send1, got1, send2, got2, send_x, recv_x, s1, r1, s2, r2, s3, r3, s_y, r_y,
):
    place = Place(n)
    groups = place.groups
    near = place.near
    count, d = resid.shape
    heads, size = norm_out.shape[1], norm_out.shape[2]
    width = wq_h.shape[0]
    experts_local = eg.shape[0]
    b_dir, c_dir = (0, 1, 0), (1, 0, 0)

    barrier = pltpu.get_barrier_semaphore()
    greeted = place.slots()[1:]
    for slot in greeted:
        pl.semaphore_signal(barrier, inc=1, device_id=place.device(slot), device_id_type=MESH)

    def loading(pairs, sems):
        copies = [pltpu.make_async_copy(src, dst, sems.at[i]) for i, (src, dst) in enumerate(pairs)]
        for copy in copies:
            copy.start()
        return copies

    small = loading(
        (
            (resid_h, resid), (gains_h, gains), (wi_h, wi), (wf_h, wf), (bi_h, bi), (bf_h, bf), (smax_h, smax),
            (routes_h, routes), (scores_h, scores), (snorm_h, snorm), (bw_h, bw),
            *[(w, wp.at[i * width : (i + 1) * width]) for i, w in enumerate((wq_h, wk_h, wv_h, wo_h))],
        ),
        load_s,
    )
    wide_d, wide_e = dg.shape[1], eg.shape[2]
    states, big = [], []

    def load_rest():
        states.extend(loading([(state_h.at[s], fresh.at[s]) for s in range(count)], load_m))
        big.extend(
            loading(
                (
                    (mix_h, mix), (dg_h, dg), (du_h, du), (eg_h, eg), (eu_h, eu), (dd_h, down.at[0:wide_d]),
                    *[
                        (ed_h.at[e], down.at[wide_d + e * wide_e : wide_d + (e + 1) * wide_e])
                        for e in range(experts_local)
                    ],
                ),
                load_w,
            )
        )

    small[0].wait()
    small[1].wait()
    normed = rms_scale(resid[...].astype(F32), gains[0:1, :])
    for half in range(2):
        rows1[0, 0, 0, half] = fold(normed[:, half * d // 2 : (half + 1) * d // 2]).astype(BF16)
    normed = normed.astype(BF16)

    gate = {}

    def column(row):
        eye = lax.broadcasted_iota(jnp.int32, (count, count), 0) == lax.broadcasted_iota(jnp.int32, (count, count), 1)
        return jnp.sum(jnp.where(eye, row, 0.0), axis=-1, keepdims=True)

    def gates():
        for copy in small[2:]:
            copy.wait()
        eye = lax.broadcasted_iota(jnp.int32, (heads, heads), 0) == lax.broadcasted_iota(jnp.int32, (heads, heads), 1)
        bias_i = jnp.sum(jnp.where(eye, bi[...], 0.0), axis=-1, keepdims=True)
        bias_f = jnp.sum(jnp.where(eye, bf[...], 0.0), axis=-1, keepdims=True)
        ipre = dot_t(wi[...], normed) + bias_i
        fpre = dot_t(wf[...], normed) + bias_f
        logf = jnp.minimum(fpre, 0.0) - jnp.log1p(jnp.exp(-jnp.abs(fpre)))
        old_max = logf + smax[...]
        new_max = jnp.maximum(ipre, old_max)
        max_out[...] = new_max
        keep, write = jnp.exp(old_max - new_max), jnp.exp(ipre - new_max)
        gate["keep"] = [column(keep[h : h + 1, :]) for h in range(heads)]
        gate["write"] = [column(write[h : h + 1, :]) for h in range(heads)]
        for h in range(heads):
            keep3[:, h, :] = jnp.broadcast_to(gate["keep"][h], (count, size))

    halved = {"at": 0}

    def halve(upto):
        for s in range(halved["at"], upto):
            states[s].wait()
            for h in range(heads):
                halves[s, h * size : (h + 1) * size, :] = fresh[s, h].astype(BF16).T
        halved["at"] = upto

    x_sent = []

    def project(rc, rb):
        piece = 0.0
        for half in range(2):
            stacked = rows1[rc, rb, :, half].reshape(groups * 2 * count, d // 4)
            for part in range(2):
                q = (2 * half + part) * d // 4
                value = dot_t(stacked, wp[:, q : q + d // 4]).reshape(groups, 2 * count, 4 * width)
                piece = piece + value[:, part * count : (part + 1) * count, :]
        code = jnp.concatenate([routes[...].astype(F32), scores[...].astype(F32)], axis=0)
        code = jnp.concatenate([code, jnp.zeros((ROWS - count, 4 * width - count), F32)], axis=1)
        for ra in range(groups):
            slot = (rc, rb, ra)
            i = (rc * 2 + rb) * groups + ra
            local[i] = jnp.concatenate([piece[ra], code], axis=0).astype(BF16)
            if i:
                x_sent.append(
                    push(local.at[i], landed.at[place.me], send_x.at[i], recv_x.at[place.me], place.device(slot))
                )
            else:
                landed[place.me] = local[0]

    def work_1(point):
        if point == "sent":
            gates()
            load_rest()
        elif point in HALVE_AT:
            halve(round(count * HALVE_AT[point]))
        elif point in PROJECT_AT:
            project(*PROJECT_AT[point])

    pl.semaphore_wait(barrier, len(greeted))
    gather(place, rows1, send1, got1, work_1, "g1")

    halve(count)
    for i, slot in enumerate(place.slots()):
        if i:
            arrived(landed.at[place.index(slot)], recv_x.at[place.index(slot)], place.device(slot))

    per_head = size // width
    numers = []
    head_of = lax.broadcasted_iota(jnp.int32, (heads, heads * size), 1) // size
    own_head = head_of == lax.broadcasted_iota(jnp.int32, (heads, heads * size), 0)

    def cell_rows(m, h):
        parts = [
            landed[h * per_head + p, :, m * width : (m + 1) * width].astype(F32)[0:count] for p in range(per_head)
        ]
        return jnp.concatenate(parts, axis=1)

    queries, keys, denoms, writes = [], [], [], []
    for h in range(heads):
        q = cell_rows(0, h)
        raw = cell_rows(1, h)
        k = raw * size ** (-0.5)
        v = cell_rows(2, h)
        new_norm = gate["keep"][h] * snorm[:, h, :] + gate["write"][h] * k
        norm_out[:, h, :] = new_norm
        denoms.append(jnp.maximum(jnp.abs(jnp.sum(new_norm * q, axis=-1, keepdims=True)), 1.0))
        writes.append(gate["write"][h] * v * jnp.sum(k * q, axis=-1, keepdims=True))
        queries.append(q)
        wv3[:, h, :] = gate["write"][h] * v * size ** (-0.5)
        keys.append(raw)
    query = jnp.concatenate(queries, axis=1)
    key_rows = jnp.concatenate(keys, axis=1)
    for s in range(count):
        krow[s] = key_rows[s : s + 1, :]
    for s in range(count):
        spread = jnp.where(own_head, query[s : s + 1, :], 0.0).astype(BF16)
        numer3[s] = dot(spread, halves[s])
    for h in range(heads):
        numer = gate["keep"][h] * numer3[:, h, :] + writes[h]
        outgate = cell_rows(3, h)
        gated[:, h * size : (h + 1) * size] = (jax.nn.sigmoid(outgate) * (numer / denoms[h])).astype(BF16)
    big[0].wait()
    mixed = dot(gated[...], mix[...])
    stream = resid[...].astype(F32) + rms_scale(mixed, gains[1:2, :])
    middle[...] = stream
    branch_in = rms_scale(stream, gains[2:3, :])
    for half in range(2):
        rows2[0, 0, 0, half] = fold(branch_in[:, half * d // 2 : (half + 1) * d // 2]).astype(BF16)

    def update(s, carry):
        value = wv3[s]
        parts = []
        for _ in range(3):
            parts.append(value.astype(BF16))
            value = value - parts[-1].astype(F32)
        key = jnp.where(own_head, krow[s], 0.0).astype(BF16)
        outer = lax.dot_general(
            jnp.concatenate(parts, axis=0), jnp.concatenate([key] * 3, axis=0),
            (((0,), (0,)), ((), ())), preferred_element_type=F32,
        )
        kept = keep3[s]
        for h in range(heads):
            fresh[s, h] = fresh[s, h] * kept[h : h + 1, :] + outer[:, h * size : (h + 1) * size]
        return carry

    def shares():
        cols = lax.broadcasted_iota(jnp.int32, (count, size), 1)
        eye = lax.broadcasted_iota(jnp.int32, (count, size), 0) == cols
        for j in range(n // 2):
            found = [[] for _ in range(experts_local)]
            for slot in place.slots()[2 * j : 2 * j + 2]:
                codes = landed[place.index(slot), :, 0:size].astype(F32)
                r0, r1 = codes[count : count + 1], codes[count + 1 : count + 2]
                c0, c1 = codes[count + 2 : count + 3], codes[count + 3 : count + 4]
                for e in range(experts_local):
                    mine = (place.me * experts_local + e).astype(F32)
                    part = (jnp.where(r0 == mine, c0, 0.0) + jnp.where(r1 == mine, c1, 0.0)) / (c0 + c1)
                    found[e].append(jnp.sum(jnp.where(eye, part, 0.0), axis=-1, keepdims=True))
            for e in range(experts_local):
                value = jnp.concatenate(found[e], axis=0)
                share[e, 2 * j * count : 2 * (j + 1) * count, :] = jnp.broadcast_to(value, (2 * count, size))

    updated = {"at": 0}

    def updates(upto):
        upto = round(count * upto)
        lax.fori_loop(updated["at"], upto, update, 0, unroll=True)
        updated["at"] = upto

    rows_half = n * count // 2

    def unfold(rb):
        for rc in range(2):
            base = (rb * 2 + rc) * groups
            for j in range(groups // 2):
                at = (base + 2 * j) * count
                for half in range(2):
                    pair = [rows2[rc, rb, 2 * j + i, half].astype(F32) for i in range(2)]
                    for part in range(2):
                        q = (2 * half + part) * d // 4
                        everything[at : at + 2 * count, q : q + d // 4] = jnp.concatenate(
                            [value[part * count : (part + 1) * count] for value in pair], axis=0
                        ).astype(BF16)

    def ups(rb):
        rows = slice(rb * rows_half, (rb + 1) * rows_half)
        logit = jnp.zeros((rows_half, size), F32)
        for j in range(d // size):
            logit = logit + everything[rows, j * size : (j + 1) * size].astype(F32) * bw[j : j + 1, :].astype(F32)
        branch_gate = jax.nn.sigmoid(jnp.sum(logit, axis=-1, keepdims=True))
        parts = [(dg, du, 0, branch_gate)]
        parts += [(eg.at[e], eu.at[e], wide_d + e * wide_e, share[e, rows, 0:1]) for e in range(experts_local)]
        for gate_w, up_w, start, scale in parts:
            wide = gate_w.shape[1]
            cut = min(256, wide)
            for j in range(wide // cut):
                cols = slice(j * cut, (j + 1) * cut)
                g = dot(everything[rows, :], gate_w[:, cols])
                u = dot(everything[rows, :], up_w[:, cols])
                hid[rows, start + j * cut : start + (j + 1) * cut] = (jax.nn.silu(g) * u * scale).astype(BF16)
                yield

    todo = {}

    def some(rb, count):
        for _ in range(count):
            next(todo[rb], None)

    wide, quarter = d // 2, n * count // 4
    downs, copies = {}, []

    def down_proj(rb):
        yield
        for copy in big[5:] if rb == 0 else []:
            copy.wait()
        for g in range(2):
            rows = slice(rb * rows_half, (rb + 1) * rows_half)
            for j in range(g * wide, (g + 1) * wide, PIECE):
                at = j - g * wide
                term[g, rb, :, at : at + PIECE] = dot(hid[rows, :], down[:, j : j + PIECE]).astype(BF16)
            downs[g, rb] = push(
                term.at[g, rb, quarter : 2 * quarter], recv1.at[g, rb], s1.at[2 * rb + g], r1.at[2 * rb + g],
                place.device(c_dir),
            )
            yield

    def work_2(point):
        if point == "sent":
            updates(0.5)
            shares()
        elif point == "near":
            unfold(0)
            for copy in big[1:5]:
                copy.wait()
            todo[0] = itertools.chain(ups(0), down_proj(0))
            some(0, AHEAD)
        elif point == "far":
            some(0, 1)
        elif point == "relayed":
            some(0, 99)
        elif point == "done":
            unfold(1)
            todo[1] = itertools.chain(ups(1), down_proj(1))

    gather(place, rows2, send2, got2, work_2, "g2")

    some(1, 99)

    def sum_c(g, rb):
        downs[g, rb].wait_recv()
        return term[g, rb, 0:quarter].astype(F32) + recv1[g, rb].astype(F32)

    def along(parts, lands, sems):
        for i, ra in enumerate(place.first):
            there = place.back(ra)
            copies.append(
                push(parts.at[ra], lands.at[there], sems[0].at[i], sems[1].at[there], place.device((0, 0, ra)))
            )

    def landed_a(value, lands, sem):
        for ra in near:
            arrived(lands.at[ra], sem.at[ra], place.device((0, 0, ra)))
        for ra in range(1, groups):
            value = value + lands[ra].astype(F32)
        return value

    value = [sum_c(0, rb) for rb in range(2)]
    for ra in range(groups):
        both = jnp.concatenate([value[rb][ra * count : (ra + 1) * count] for rb in range(2)], axis=0)
        if ra:
            part_z[ra] = both.astype(BF16)
        else:
            own_z[...] = both
    along(part_z, recv_z, (s2, r2))
    part_y[...] = sum_c(1, 1).astype(BF16)
    own_y[...] = sum_c(1, 0)
    swap_y = push(part_y, recv_y, s_y.at[0], r_y.at[0], place.device(b_dir))
    updates(0.7)
    swap_y.wait_recv()
    value = own_y[...] + recv_y[...].astype(F32)
    for ra in range(1, groups):
        part_yz[ra] = fold(value[ra * count : (ra + 1) * count]).astype(BF16)
    along(part_yz, recv_yz, (s3, r3))
    finals = [None, fold(value[0:count])]
    value = landed_a(own_z[...], recv_z, r2)
    part_zy[...] = fold(value[count:]).astype(BF16)
    finals[0] = fold(value[0:count])
    swap_z = push(part_zy, recv_zy, s_y.at[1], r_y.at[1], place.device(b_dir))
    updates(1)
    finals[1] = landed_a(finals[1], recv_yz, r3)
    swap_z.wait_recv()
    finals[0] = finals[0] + recv_zy[...].astype(F32)
    square = sum(jnp.sum(value * value, axis=-1, keepdims=True) for value in finals)
    scale = lax.rsqrt((square[0:count] + square[count:]) / d + 1e-06)
    for g in range(2):
        for part in range(2):
            cols = slice(g * wide + part * wide // 2, g * wide + (part + 1) * wide // 2)
            extra = finals[g][part * count : (part + 1) * count] * scale * gains[3:4, cols]
            out_ref[:, cols] = (middle[:, cols] + extra).astype(BF16)
    for copy in x_sent + list(downs.values()) + [swap_y, swap_z] + copies:
        copy.wait_send()


def finish_kernel(fresh, norm, top, out, fresh_o, norm_o, top_o, out_o, sems):
    count = fresh.shape[0]
    pairs = [(out, out_o), (norm, norm_o), (top, top_o)] + [(fresh.at[s], fresh_o.at[s]) for s in range(count)]
    copies = [pltpu.make_async_copy(src, dst, sems.at[i]) for i, (src, dst) in enumerate(pairs)]
    for copy in copies:
        copy.start()
    for copy in copies:
        copy.wait()


def local(
    resid, norm_gains, w_query, w_key, w_value, w_outgate, w_igate, w_fgate,
    igate_bias, fgate_bias, state_matrix, state_norm, state_max, w_mix_out,
    routes, route_scores, expert_gate, expert_up, expert_down,
    dense_gate, dense_up, dense_down, branch_weight,
):
    n = lax.axis_size("ep")
    groups = n // 4
    count, d = resid.shape
    _, heads, size, _ = state_matrix.shape
    width = w_query.shape[1]
    experts = expert_gate.shape[0]
    hidden = dense_gate.shape[1] + experts * expert_gate.shape[2]
    wide = d // 2
    quarter = n * count // 4
    args = [
        resid, norm_gains, w_query.T, w_key.T, w_value.T, w_outgate.T, w_igate.T, w_fgate.T,
        igate_bias[None], fgate_bias[None], state_max.T, state_norm, state_matrix, w_mix_out,
        routes.T, route_scores.T, expert_gate, expert_up, expert_down, dense_gate, dense_up, dense_down,
        branch_weight.reshape(d // size, size),
    ]
    args = [pltpu.with_memory_space_constraint(x, pltpu.HBM) for x in args]
    vmem = pl.BlockSpec(memory_space=pltpu.VMEM)
    hbm = pl.BlockSpec(memory_space=pltpu.HBM)
    kept = (
        pltpu.VMEM(state_matrix.shape, F32),
        pltpu.VMEM(state_norm.shape, F32),
        pltpu.VMEM((heads, count), F32),
        pltpu.VMEM((count, d), BF16),
    )
    small = pltpu.VMEM((count, heads, size), F32)
    results = pl.pallas_call(
        functools.partial(step_kernel, n),
        out_shape=kept,
        in_specs=[hbm] * len(args),
        out_specs=(vmem,) * 4,
        scratch_shapes=[
            pltpu.VMEM((count, d), BF16),
            pltpu.VMEM(norm_gains.shape, F32),
            pltpu.VMEM((4 * width, d), BF16),
            pltpu.VMEM((heads, d), BF16),
            pltpu.VMEM((heads, d), BF16),
            pltpu.VMEM((1, heads), F32),
            pltpu.VMEM((1, heads), F32),
            pltpu.VMEM((heads, count), F32),
            pltpu.VMEM(state_norm.shape, F32),
            pltpu.VMEM((routes.shape[1], count), jnp.int32),
            pltpu.VMEM((routes.shape[1], count), BF16),
            pltpu.VMEM((d // size, size), BF16),
            pltpu.VMEM(w_mix_out.shape, BF16),
            pltpu.VMEM(expert_gate.shape, BF16),
            pltpu.VMEM(expert_up.shape, BF16),
            pltpu.VMEM(dense_gate.shape, BF16),
            pltpu.VMEM(dense_up.shape, BF16),
            pltpu.VMEM((hidden, d), BF16),
            pltpu.VMEM((2, 2, groups, 2, 2 * count, d // 4), BF16),
            pltpu.VMEM((2, 2, groups, 2, 2 * count, d // 4), BF16),
            pltpu.VMEM((n, ROWS, 4 * width), BF16),
            pltpu.VMEM((n, ROWS, 4 * width), BF16),
            pltpu.VMEM((count, heads * size, size), BF16),
            pltpu.VMEM((count, 1, heads * size), F32),
            small, small, small,
            pltpu.VMEM((count, heads * size), BF16),
            pltpu.VMEM((count, d), F32),
            pltpu.VMEM((experts, n * count, size), F32),
            pltpu.VMEM((n * count, d), BF16),
            pltpu.VMEM((n * count, hidden), BF16),
            pltpu.VMEM((2, 2, 2 * quarter, wide), BF16),
            pltpu.VMEM((2, 2, quarter, wide), BF16),
            pltpu.VMEM((groups, 2 * count, wide), BF16),
            pltpu.VMEM((groups, 2 * count, wide), BF16),
            pltpu.VMEM((2 * count, wide), F32),
            pltpu.VMEM((2 * count, wide // 2), BF16),
            pltpu.VMEM((2 * count, wide // 2), BF16),
            pltpu.VMEM((quarter, wide), BF16),
            pltpu.VMEM((quarter, wide), BF16),
            pltpu.VMEM((quarter, wide), F32),
            pltpu.VMEM((groups, 2 * count, wide // 2), BF16),
            pltpu.VMEM((groups, 2 * count, wide // 2), BF16),
            DMA((15,)),
            DMA((count,)),
            DMA((6 + experts,)),
            DMA((10 * groups,)),
            DMA((2, 2, groups, 2)),
            DMA((10 * groups,)),
            DMA((2, 2, groups, 2)),
            DMA((n,)),
            DMA((n,)),
            DMA((CHUNKS,)),
            DMA((CHUNKS,)),
            DMA((groups,)),
            DMA((groups,)),
            DMA((groups,)),
            DMA((groups,)),
            DMA((2,)),
            DMA((2,)),
        ],
        compiler_params=pltpu.CompilerParams(
            collective_id=0, has_side_effects=True, vmem_limit_bytes=STEP_VMEM
        ),
        name="step",
    )(*args)
    new_matrix, new_norm, new_max, out_stream = pl.pallas_call(
        finish_kernel,
        out_shape=(
            jax.ShapeDtypeStruct(state_matrix.shape, F32),
            jax.ShapeDtypeStruct(state_norm.shape, F32),
            jax.ShapeDtypeStruct((heads, count), F32),
            jax.ShapeDtypeStruct((count, d), BF16),
        ),
        in_specs=[vmem] * 4,
        out_specs=(hbm,) * 4,
        scratch_shapes=[DMA((3 + count,))],
        compiler_params=pltpu.CompilerParams(vmem_limit_bytes=2**20),
        name="finish",
    )(*results)
    return (out_stream, new_matrix, new_norm, new_max.T)


def solution(mesh):
    rows = ("grp", "ep")
    placed = (
        P(rows, None),
        P(),
        P(None, "ep"),
        P(None, "ep"),
        P(None, "ep"),
        P(None, "ep"),
        P(),
        P(),
        P(),
        P(),
        P(rows, None, None, None),
        P(rows, None, None),
        P(rows, None),
        P(),
        P(rows, None),
        P(rows, None),
        P("ep", None, None),
        P("ep", None, None),
        P("ep", None, None),
        P(None, "ep"),
        P(None, "ep"),
        P("ep", None),
        P(),
    )
    return jax.shard_map(
        local,
        mesh=mesh,
        in_specs=placed,
        out_specs=(
            P(rows, None),
            P(rows, None, None, None),
            P(rows, None, None),
            P(rows, None),
        ),
        check_vma=False,
    )
```

```python
import functools
import itertools

import jax
import jax.numpy as jnp
from jax import lax
from jax.experimental import pallas as pl
from jax.experimental.pallas import tpu as pltpu
from jax.sharding import PartitionSpec as P

MESH = pl.DeviceIdType.MESH
F32 = jnp.float32
BF16 = jnp.bfloat16
ROWS = 16
STEP_VMEM = 50 * 2**20
CHUNKS = 4
PIECE = 256
AHEAD = 3
HALVE_AT = {"first": 0.25, "second": 0.25, "third": 0.5}
PROJECT_AT = {"sides": (0, 0), "near": (1, 0), "relayed": (0, 1), "done": (1, 1)}
DMA = pltpu.SemaphoreType.DMA


def rms_scale(values, gains):
    return values * lax.rsqrt(jnp.mean(values * values, axis=-1, keepdims=True) + 1e-06) * gains


def dot_t(left, right):
    return lax.dot_general(left, right, (((1,), (1,)), ((), ())), preferred_element_type=F32)


def dot(left, right):
    return jnp.dot(left, right, preferred_element_type=F32)


def fold(values):
    half = values.shape[1] // 2
    return jnp.concatenate([values[:, :half], values[:, half:]], axis=0)


class Place:
    def __init__(self, n):
        self.n, self.groups = n, n // 4
        self.me = lax.axis_index("ep")
        self.a, self.b, self.c = lax.div(self.me, 4), lax.rem(lax.div(self.me, 2), 2), lax.rem(self.me, 2)
        far = self.groups - 1
        self.near = [self.ranked(i, lambda k, a: (abs(k - a), -abs(2 * k - far))) for i in range(far)]
        self.first = [self.ranked(i, lambda k, a: k) for i in range(self.groups - 1)]

    def ranked(self, i, rank):
        ahead = 0
        for a in range(self.groups):
            others = sorted((k for k in range(self.groups) if k != a), key=lambda k: (rank(k, a), k))
            ahead = jnp.where(self.a == a, (others[i] - a) % self.groups, ahead)
        return ahead

    def back(self, ra):
        return lax.rem(self.groups - ra, self.groups)

    def index(self, slot):
        rc, rb, ra = slot
        a = self.a if isinstance(ra, int) and ra == 0 else lax.rem(self.a + ra, self.groups)
        b = 1 - self.b if rb else self.b
        c = 1 - self.c if rc else self.c
        return (a * 2 + b) * 2 + c

    def device(self, slot):
        return {"ep": self.index(slot)}

    def slots(self):
        return [(rc, rb, ra) for rb in range(2) for rc in range(2) for ra in range(self.groups)]


def push(src, dst, send_sem, recv_sem, to):
    copy = pltpu.make_async_remote_copy(
        src_ref=src, dst_ref=dst, send_sem=send_sem, recv_sem=recv_sem,
        device_id=to, device_id_type=MESH,
    )
    copy.start()
    return copy


def arrived(dst, sem, to):
    pltpu.make_async_remote_copy(
        src_ref=dst, dst_ref=dst, send_sem=sem, recv_sem=sem, device_id=to, device_id_type=MESH,
    ).wait_recv()


def gather(place, buf, send, recv, work, tag):
    groups, near = place.groups, place.near
    a_dirs, b_dir, c_dir = near, (0, 1, 0), (1, 0, 0)
    sent = []

    def ship(slot, half, there, to):
        block, far = buf.at[(*slot, half)], (*there, half)
        sent.append(push(block, buf.at[far], send.at[len(sent)], recv.at[far], place.device(to)))

    def along(rb, half, order):
        for ra in order:
            ship((0, rb, 0), half, (0, rb, place.back(ra)), (0, 0, ra))

    def across(slot, half, to):
        rc, rb, ra = slot
        ship(slot, half, (rc ^ to[0], rb ^ to[1], ra), to)

    def wait(slot, half):
        arrived(buf.at[(*slot, half)], recv.at[(*slot, half)], place.device(c_dir))

    across((0, 0, 0), 1, b_dir)
    along(0, 0, near[::-1])
    along(0, 1, near[::-1])
    across((0, 0, 0), 0, b_dir)
    across((0, 0, 0), 0, c_dir)
    across((0, 0, 0), 1, c_dir)
    work("sent")

    def own_side(i, half):
        slot = (0, 0, near[i])
        wait(slot, half)
        if half == 0:
            across(slot, half, b_dir)
        across(slot, half, c_dir)

    def other_side(slot, half, own=False):
        wait(slot, half)
        if own and half == 1:
            along(1, 1, near)
        across(slot, half, c_dir)

    last = groups - 2
    other_side((0, 1, 0), 1, own=True)
    own_side(0, 0)
    other_side((0, 1, 0), 0)
    work("first")
    for i in range(1, groups):
        if i <= last:
            own_side(i, 0)
        own_side(i - 1, 1)
        if i < groups - 1:
            work("second" if i == 1 else "third")
    work("sides")
    for ra in range(groups):
        for half in range(2):
            wait((1, 0, ra), half)
    work("near")
    for i in range(groups - 1):
        for half in (1, 0):
            other_side((0, 1, near[i]), half)
        work("far")
    work("relayed")
    for ra in range(groups):
        for half in range(2):
            wait((1, 1, ra), half)
    work("done")
    for copy in sent:
        copy.wait_send()


def step_kernel(
    n, resid_h, gains_h, wq_h, wk_h, wv_h, wo_h, wi_h, wf_h, bi_h, bf_h, smax_h, snorm_h, state_h, mix_h,
    routes_h, scores_h, eg_h, eu_h, ed_h, dg_h, du_h, dd_h, bw_h,
    fresh, norm_out, max_out, out_ref,
    resid, gains, wp, wi, wf, bi, bf, smax, snorm, routes, scores, bw, mix, eg, eu, dg, du, down,
    rows1, rows2, local, landed, halves, krow, wv3, keep3, numer3, gated, middle, share, everything, hid,
    term, recv1, part_z, recv_z, own_z, part_zy, recv_zy, part_y, recv_y, own_y, part_yz, recv_yz,
    load_s, load_m, load_w, send1, got1, send2, got2, send_x, recv_x, s1, r1, s2, r2, s3, r3, s_y, r_y,
):
    place = Place(n)
    groups = place.groups
    near = place.near
    count, d = resid.shape
    heads, size = norm_out.shape[1], norm_out.shape[2]
    width = wq_h.shape[0]
    experts_local = eg.shape[0]
    b_dir, c_dir = (0, 1, 0), (1, 0, 0)

    barrier = pltpu.get_barrier_semaphore()
    greeted = [(0, 0, ra) for ra in range(1, groups)] + [b_dir, c_dir]
    for slot in greeted:
        pl.semaphore_signal(barrier, inc=1, device_id=place.device(slot), device_id_type=MESH)

    def loading(pairs, sems):
        copies = [pltpu.make_async_copy(src, dst, sems.at[i]) for i, (src, dst) in enumerate(pairs)]
        for copy in copies:
            copy.start()
        return copies

    small = loading(
        (
            (resid_h, resid), (gains_h, gains), (wi_h, wi), (wf_h, wf), (bi_h, bi), (bf_h, bf), (smax_h, smax),
            (routes_h, routes), (scores_h, scores), (snorm_h, snorm), (bw_h, bw),
            *[(w, wp.at[i * width : (i + 1) * width]) for i, w in enumerate((wq_h, wk_h, wv_h, wo_h))],
        ),
        load_s,
    )
    wide_d, wide_e = dg.shape[1], eg.shape[2]
    states, big = [], []

    def load_rest():
        states.extend(loading([(state_h.at[s], fresh.at[s]) for s in range(count)], load_m))
        big.extend(
            loading(
                (
                    (mix_h, mix), (dg_h, dg), (du_h, du), (eg_h, eg), (eu_h, eu), (dd_h, down.at[0:wide_d]),
                    *[
                        (ed_h.at[e], down.at[wide_d + e * wide_e : wide_d + (e + 1) * wide_e])
                        for e in range(experts_local)
                    ],
                ),
                load_w,
            )
        )

    small[0].wait()
    small[1].wait()
    normed = rms_scale(resid[...].astype(F32), gains[0:1, :])
    for half in range(2):
        rows1[0, 0, 0, half] = fold(normed[:, half * d // 2 : (half + 1) * d // 2]).astype(BF16)
    normed = normed.astype(BF16)

    gate = {}

    def column(row):
        eye = lax.broadcasted_iota(jnp.int32, (count, count), 0) == lax.broadcasted_iota(jnp.int32, (count, count), 1)
        return jnp.sum(jnp.where(eye, row, 0.0), axis=-1, keepdims=True)

    def gates():
        for copy in small[2:]:
            copy.wait()
        eye = lax.broadcasted_iota(jnp.int32, (heads, heads), 0) == lax.broadcasted_iota(jnp.int32, (heads, heads), 1)
        bias_i = jnp.sum(jnp.where(eye, bi[...], 0.0), axis=-1, keepdims=True)
        bias_f = jnp.sum(jnp.where(eye, bf[...], 0.0), axis=-1, keepdims=True)
        ipre = dot_t(wi[...], normed) + bias_i
        fpre = dot_t(wf[...], normed) + bias_f
        logf = jnp.minimum(fpre, 0.0) - jnp.log1p(jnp.exp(-jnp.abs(fpre)))
        old_max = logf + smax[...]
        new_max = jnp.maximum(ipre, old_max)
        max_out[...] = new_max
        keep, write = jnp.exp(old_max - new_max), jnp.exp(ipre - new_max)
        gate["keep"] = [column(keep[h : h + 1, :]) for h in range(heads)]
        gate["write"] = [column(write[h : h + 1, :]) for h in range(heads)]
        for h in range(heads):
            keep3[:, h, :] = jnp.broadcast_to(gate["keep"][h], (count, size))

    halved = {"at": 0}

    def halve(upto):
        for s in range(halved["at"], upto):
            states[s].wait()
            for h in range(heads):
                halves[s, h * size : (h + 1) * size, :] = fresh[s, h].astype(BF16).T
        halved["at"] = upto

    x_sent = []

    def project(rc, rb):
        piece = 0.0
        for half in range(2):
            stacked = rows1[rc, rb, :, half].reshape(groups * 2 * count, d // 4)
            for part in range(2):
                q = (2 * half + part) * d // 4
                value = dot_t(stacked, wp[:, q : q + d // 4]).reshape(groups, 2 * count, 4 * width)
                piece = piece + value[:, part * count : (part + 1) * count, :]
        code = jnp.concatenate([routes[...].astype(F32), scores[...].astype(F32)], axis=0)
        code = jnp.concatenate([code, jnp.zeros((ROWS - count, 4 * width - count), F32)], axis=1)
        for ra in range(groups):
            slot = (rc, rb, ra)
            i = (rc * 2 + rb) * groups + ra
            local[i] = jnp.concatenate([piece[ra], code], axis=0).astype(BF16)
            if i:
                x_sent.append(
                    push(local.at[i], landed.at[place.me], send_x.at[i], recv_x.at[place.me], place.device(slot))
                )
            else:
                landed[place.me] = local[0]

    def work_1(point):
        if point == "sent":
            gates()
            load_rest()
        elif point in HALVE_AT:
            halve(round(count * HALVE_AT[point]))
        elif point in PROJECT_AT:
            project(*PROJECT_AT[point])

    pl.semaphore_wait(barrier, len(greeted))
    gather(place, rows1, send1, got1, work_1, "g1")

    halve(count)
    for i, slot in enumerate(place.slots()):
        if i:
            arrived(landed.at[place.index(slot)], recv_x.at[place.index(slot)], place.device(slot))

    per_head = size // width
    numers = []
    head_of = lax.broadcasted_iota(jnp.int32, (heads, heads * size), 1) // size
    own_head = head_of == lax.broadcasted_iota(jnp.int32, (heads, heads * size), 0)

    def cell_rows(m, h):
        parts = [
            landed[h * per_head + p, :, m * width : (m + 1) * width].astype(F32)[0:count] for p in range(per_head)
        ]
        return jnp.concatenate(parts, axis=1)

    queries, keys, denoms, writes = [], [], [], []
    for h in range(heads):
        q = cell_rows(0, h)
        raw = cell_rows(1, h)
        k = raw * size ** (-0.5)
        v = cell_rows(2, h)
        new_norm = gate["keep"][h] * snorm[:, h, :] + gate["write"][h] * k
        norm_out[:, h, :] = new_norm
        denoms.append(jnp.maximum(jnp.abs(jnp.sum(new_norm * q, axis=-1, keepdims=True)), 1.0))
        writes.append(gate["write"][h] * v * jnp.sum(k * q, axis=-1, keepdims=True))
        queries.append(q)
        wv3[:, h, :] = gate["write"][h] * v * size ** (-0.5)
        keys.append(raw)
    query = jnp.concatenate(queries, axis=1)
    key_rows = jnp.concatenate(keys, axis=1)
    for s in range(count):
        krow[s] = key_rows[s : s + 1, :]
    for s in range(count):
        spread = jnp.where(own_head, query[s : s + 1, :], 0.0).astype(BF16)
        numer3[s] = dot(spread, halves[s])
    for h in range(heads):
        numer = gate["keep"][h] * numer3[:, h, :] + writes[h]
        outgate = cell_rows(3, h)
        gated[:, h * size : (h + 1) * size] = (jax.nn.sigmoid(outgate) * (numer / denoms[h])).astype(BF16)
    big[0].wait()
    mixed = dot(gated[...], mix[...])
    stream = resid[...].astype(F32) + rms_scale(mixed, gains[1:2, :])
    middle[...] = stream
    branch_in = rms_scale(stream, gains[2:3, :])
    for half in range(2):
        rows2[0, 0, 0, half] = fold(branch_in[:, half * d // 2 : (half + 1) * d // 2]).astype(BF16)

    def update(s, carry):
        value = wv3[s]
        parts = []
        for _ in range(3):
            parts.append(value.astype(BF16))
            value = value - parts[-1].astype(F32)
        key = jnp.where(own_head, krow[s], 0.0).astype(BF16)
        outer = lax.dot_general(
            jnp.concatenate(parts, axis=0), jnp.concatenate([key] * 3, axis=0),
            (((0,), (0,)), ((), ())), preferred_element_type=F32,
        )
        kept = keep3[s]
        for h in range(heads):
            fresh[s, h] = fresh[s, h] * kept[h : h + 1, :] + outer[:, h * size : (h + 1) * size]
        return carry

    def shares():
        cols = lax.broadcasted_iota(jnp.int32, (count, size), 1)
        eye = lax.broadcasted_iota(jnp.int32, (count, size), 0) == cols
        for j in range(n // 2):
            found = [[] for _ in range(experts_local)]
            for slot in place.slots()[2 * j : 2 * j + 2]:
                codes = landed[place.index(slot), :, 0:size].astype(F32)
                r0, r1 = codes[count : count + 1], codes[count + 1 : count + 2]
                c0, c1 = codes[count + 2 : count + 3], codes[count + 3 : count + 4]
                for e in range(experts_local):
                    mine = (place.me * experts_local + e).astype(F32)
                    part = (jnp.where(r0 == mine, c0, 0.0) + jnp.where(r1 == mine, c1, 0.0)) / (c0 + c1)
                    found[e].append(jnp.sum(jnp.where(eye, part, 0.0), axis=-1, keepdims=True))
            for e in range(experts_local):
                value = jnp.concatenate(found[e], axis=0)
                share[e, 2 * j * count : 2 * (j + 1) * count, :] = jnp.broadcast_to(value, (2 * count, size))

    updated = {"at": 0}

    def updates(upto):
        upto = round(count * upto)
        lax.fori_loop(updated["at"], upto, update, 0, unroll=True)
        updated["at"] = upto

    rows_half = n * count // 2

    def unfold(rb):
        for rc in range(2):
            base = (rb * 2 + rc) * groups
            for j in range(groups // 2):
                at = (base + 2 * j) * count
                for half in range(2):
                    pair = [rows2[rc, rb, 2 * j + i, half].astype(F32) for i in range(2)]
                    for part in range(2):
                        q = (2 * half + part) * d // 4
                        everything[at : at + 2 * count, q : q + d // 4] = jnp.concatenate(
                            [value[part * count : (part + 1) * count] for value in pair], axis=0
                        ).astype(BF16)

    def ups(rb):
        rows = slice(rb * rows_half, (rb + 1) * rows_half)
        logit = jnp.zeros((rows_half, size), F32)
        for j in range(d // size):
            logit = logit + everything[rows, j * size : (j + 1) * size].astype(F32) * bw[j : j + 1, :].astype(F32)
        branch_gate = jax.nn.sigmoid(jnp.sum(logit, axis=-1, keepdims=True))
        parts = [(dg, du, 0, branch_gate)]
        parts += [(eg.at[e], eu.at[e], wide_d + e * wide_e, share[e, rows, 0:1]) for e in range(experts_local)]
        for gate_w, up_w, start, scale in parts:
            wide = gate_w.shape[1]
            cut = min(256, wide)
            for j in range(wide // cut):
                cols = slice(j * cut, (j + 1) * cut)
                g = dot(everything[rows, :], gate_w[:, cols])
                u = dot(everything[rows, :], up_w[:, cols])
                hid[rows, start + j * cut : start + (j + 1) * cut] = (jax.nn.silu(g) * u * scale).astype(BF16)
                yield

    todo = {}

    def some(rb, count):
        for _ in range(count):
            next(todo[rb], None)

    wide, quarter = d // 2, n * count // 4
    downs, copies = {}, []

    def down_proj(rb):
        yield
        for copy in big[5:] if rb == 0 else []:
            copy.wait()
        for g in range(2):
            rows = slice(rb * rows_half, (rb + 1) * rows_half)
            for j in range(g * wide, (g + 1) * wide, PIECE):
                at = j - g * wide
                term[g, rb, :, at : at + PIECE] = dot(hid[rows, :], down[:, j : j + PIECE]).astype(BF16)
            downs[g, rb] = push(
                term.at[g, rb, quarter : 2 * quarter], recv1.at[g, rb], s1.at[2 * rb + g], r1.at[2 * rb + g],
                place.device(c_dir),
            )
            yield

    def work_2(point):
        if point == "sent":
            updates(0.5)
            shares()
        elif point == "near":
            unfold(0)
            for copy in big[1:5]:
                copy.wait()
            todo[0] = itertools.chain(ups(0), down_proj(0))
            some(0, AHEAD)
        elif point == "far":
            some(0, 1)
        elif point == "relayed":
            some(0, 99)
        elif point == "done":
            unfold(1)
            todo[1] = itertools.chain(ups(1), down_proj(1))

    gather(place, rows2, send2, got2, work_2, "g2")

    some(1, 99)

    def sum_c(g, rb):
        downs[g, rb].wait_recv()
        return term[g, rb, 0:quarter].astype(F32) + recv1[g, rb].astype(F32)

    def along(parts, lands, sems):
        for i, ra in enumerate(place.first):
            there = place.back(ra)
            copies.append(
                push(parts.at[ra], lands.at[there], sems[0].at[i], sems[1].at[there], place.device((0, 0, ra)))
            )

    def landed_a(value, lands, sem):
        for ra in near:
            arrived(lands.at[ra], sem.at[ra], place.device((0, 0, ra)))
        for ra in range(1, groups):
            value = value + lands[ra].astype(F32)
        return value

    value = [sum_c(0, rb) for rb in range(2)]
    for ra in range(groups):
        both = jnp.concatenate([value[rb][ra * count : (ra + 1) * count] for rb in range(2)], axis=0)
        if ra:
            part_z[ra] = both.astype(BF16)
        else:
            own_z[...] = both
    along(part_z, recv_z, (s2, r2))
    part_y[...] = sum_c(1, 1).astype(BF16)
    own_y[...] = sum_c(1, 0)
    swap_y = push(part_y, recv_y, s_y.at[0], r_y.at[0], place.device(b_dir))
    updates(0.7)
    swap_y.wait_recv()
    value = own_y[...] + recv_y[...].astype(F32)
    for ra in range(1, groups):
        part_yz[ra] = fold(value[ra * count : (ra + 1) * count]).astype(BF16)
    along(part_yz, recv_yz, (s3, r3))
    finals = [None, fold(value[0:count])]
    value = landed_a(own_z[...], recv_z, r2)
    part_zy[...] = fold(value[count:]).astype(BF16)
    finals[0] = fold(value[0:count])
    swap_z = push(part_zy, recv_zy, s_y.at[1], r_y.at[1], place.device(b_dir))
    updates(1)
    finals[1] = landed_a(finals[1], recv_yz, r3)
    swap_z.wait_recv()
    finals[0] = finals[0] + recv_zy[...].astype(F32)
    square = sum(jnp.sum(value * value, axis=-1, keepdims=True) for value in finals)
    scale = lax.rsqrt((square[0:count] + square[count:]) / d + 1e-06)
    for g in range(2):
        for part in range(2):
            cols = slice(g * wide + part * wide // 2, g * wide + (part + 1) * wide // 2)
            extra = finals[g][part * count : (part + 1) * count] * scale * gains[3:4, cols]
            out_ref[:, cols] = (middle[:, cols] + extra).astype(BF16)
    for copy in x_sent + list(downs.values()) + [swap_y, swap_z] + copies:
        copy.wait_send()


def finish_kernel(fresh, norm, top, out, fresh_o, norm_o, top_o, out_o, sems):
    count = fresh.shape[0]
    pairs = [(fresh.at[s], fresh_o.at[s]) for s in range(count)] + [(out, out_o), (norm, norm_o), (top, top_o)]
    copies = [pltpu.make_async_copy(src, dst, sems.at[i]) for i, (src, dst) in enumerate(pairs)]
    for copy in copies:
        copy.start()
    for copy in copies:
        copy.wait()


def local(
    resid, norm_gains, w_query, w_key, w_value, w_outgate, w_igate, w_fgate,
    igate_bias, fgate_bias, state_matrix, state_norm, state_max, w_mix_out,
    routes, route_scores, expert_gate, expert_up, expert_down,
    dense_gate, dense_up, dense_down, branch_weight,
):
    n = lax.axis_size("ep")
    groups = n // 4
    count, d = resid.shape
    _, heads, size, _ = state_matrix.shape
    width = w_query.shape[1]
    experts = expert_gate.shape[0]
    hidden = dense_gate.shape[1] + experts * expert_gate.shape[2]
    wide = d // 2
    quarter = n * count // 4
    args = [
        resid, norm_gains, w_query.T, w_key.T, w_value.T, w_outgate.T, w_igate.T, w_fgate.T,
        igate_bias[None], fgate_bias[None], state_max.T, state_norm, state_matrix, w_mix_out,
        routes.T, route_scores.T, expert_gate, expert_up, expert_down, dense_gate, dense_up, dense_down,
        branch_weight.reshape(d // size, size),
    ]
    args = [pltpu.with_memory_space_constraint(x, pltpu.HBM) for x in args]
    vmem = pl.BlockSpec(memory_space=pltpu.VMEM)
    hbm = pl.BlockSpec(memory_space=pltpu.HBM)
    kept = (
        pltpu.VMEM(state_matrix.shape, F32),
        pltpu.VMEM(state_norm.shape, F32),
        pltpu.VMEM((heads, count), F32),
        pltpu.VMEM((count, d), BF16),
    )
    small = pltpu.VMEM((count, heads, size), F32)
    results = pl.pallas_call(
        functools.partial(step_kernel, n),
        out_shape=kept,
        in_specs=[hbm] * len(args),
        out_specs=(vmem,) * 4,
        scratch_shapes=[
            pltpu.VMEM((count, d), BF16),
            pltpu.VMEM(norm_gains.shape, F32),
            pltpu.VMEM((4 * width, d), BF16),
            pltpu.VMEM((heads, d), BF16),
            pltpu.VMEM((heads, d), BF16),
            pltpu.VMEM((1, heads), F32),
            pltpu.VMEM((1, heads), F32),
            pltpu.VMEM((heads, count), F32),
            pltpu.VMEM(state_norm.shape, F32),
            pltpu.VMEM((routes.shape[1], count), jnp.int32),
            pltpu.VMEM((routes.shape[1], count), BF16),
            pltpu.VMEM((d // size, size), BF16),
            pltpu.VMEM(w_mix_out.shape, BF16),
            pltpu.VMEM(expert_gate.shape, BF16),
            pltpu.VMEM(expert_up.shape, BF16),
            pltpu.VMEM(dense_gate.shape, BF16),
            pltpu.VMEM(dense_up.shape, BF16),
            pltpu.VMEM((hidden, d), BF16),
            pltpu.VMEM((2, 2, groups, 2, 2 * count, d // 4), BF16),
            pltpu.VMEM((2, 2, groups, 2, 2 * count, d // 4), BF16),
            pltpu.VMEM((n, ROWS, 4 * width), BF16),
            pltpu.VMEM((n, ROWS, 4 * width), BF16),
            pltpu.VMEM((count, heads * size, size), BF16),
            pltpu.VMEM((count, 1, heads * size), F32),
            small, small, small,
            pltpu.VMEM((count, heads * size), BF16),
            pltpu.VMEM((count, d), F32),
            pltpu.VMEM((experts, n * count, size), F32),
            pltpu.VMEM((n * count, d), BF16),
            pltpu.VMEM((n * count, hidden), BF16),
            pltpu.VMEM((2, 2, 2 * quarter, wide), BF16),
            pltpu.VMEM((2, 2, quarter, wide), BF16),
            pltpu.VMEM((groups, 2 * count, wide), BF16),
            pltpu.VMEM((groups, 2 * count, wide), BF16),
            pltpu.VMEM((2 * count, wide), F32),
            pltpu.VMEM((2 * count, wide // 2), BF16),
            pltpu.VMEM((2 * count, wide // 2), BF16),
            pltpu.VMEM((quarter, wide), BF16),
            pltpu.VMEM((quarter, wide), BF16),
            pltpu.VMEM((quarter, wide), F32),
            pltpu.VMEM((groups, 2 * count, wide // 2), BF16),
            pltpu.VMEM((groups, 2 * count, wide // 2), BF16),
            DMA((15,)),
            DMA((count,)),
            DMA((6 + experts,)),
            DMA((10 * groups,)),
            DMA((2, 2, groups, 2)),
            DMA((10 * groups,)),
            DMA((2, 2, groups, 2)),
            DMA((n,)),
            DMA((n,)),
            DMA((CHUNKS,)),
            DMA((CHUNKS,)),
            DMA((groups,)),
            DMA((groups,)),
            DMA((groups,)),
            DMA((groups,)),
            DMA((2,)),
            DMA((2,)),
        ],
        compiler_params=pltpu.CompilerParams(
            collective_id=0, has_side_effects=True, vmem_limit_bytes=STEP_VMEM
        ),
        name="step",
    )(*args)
    new_matrix, new_norm, new_max, out_stream = pl.pallas_call(
        finish_kernel,
        out_shape=(
            jax.ShapeDtypeStruct(state_matrix.shape, F32),
            jax.ShapeDtypeStruct(state_norm.shape, F32),
            jax.ShapeDtypeStruct((heads, count), F32),
            jax.ShapeDtypeStruct((count, d), BF16),
        ),
        in_specs=[vmem] * 4,
        out_specs=(hbm,) * 4,
        scratch_shapes=[DMA((3 + count,))],
        compiler_params=pltpu.CompilerParams(vmem_limit_bytes=2**20),
        name="finish",
    )(*results)
    return (out_stream, new_matrix, new_norm, new_max.T)


def solution(mesh):
    rows = ("grp", "ep")
    placed = (
        P(rows, None),
        P(),
        P(None, "ep"),
        P(None, "ep"),
        P(None, "ep"),
        P(None, "ep"),
        P(),
        P(),
        P(),
        P(),
        P(rows, None, None, None),
        P(rows, None, None),
        P(rows, None),
        P(),
        P(rows, None),
        P(rows, None),
        P("ep", None, None),
        P("ep", None, None),
        P("ep", None, None),
        P(None, "ep"),
        P(None, "ep"),
        P("ep", None),
        P(),
    )
    return jax.shard_map(
        local,
        mesh=mesh,
        in_specs=placed,
        out_specs=(
            P(rows, None),
            P(rows, None, None, None),
            P(rows, None, None),
            P(rows, None),
        ),
        check_vma=False,
    )
```
